256 devices in a mesh: sp: 32 (over z, x), tp: 8 (over y, core).
Axes of the slice: x: 4, y: 4, z: 8, core: 2. Of those that a mesh axis runs over, the one named last changes fastest.
Arguments:
- residual: bfloat16 [10240, 2048], P(('sp', 'tp')), may hold values from -6 to 6
- query_narrow: bfloat16 [10240, 1024], P('sp', 'tp'), may hold values from -48 to 48
- key_narrow: bfloat16 [10240, 1024], P('sp', 'tp'), may hold values from -48 to 48
- value_narrow: bfloat16 [10240, 1024], P('sp', 'tp'), may hold values from -6 to 6
- query_wide: bfloat16 [10240, 2048], P('sp', 'tp'), may hold values from -48 to 48
- key_wide: bfloat16 [10240, 2048], P('sp', 'tp'), may hold values from -48 to 48
- value_wide: bfloat16 [10240, 1024], P('sp', 'tp'), may hold values from -6 to 6
- subtract_narrow: float32 [8], P('tp'), may hold values from 0.3 to 0.8
- subtract_wide: float32 [8], P('tp'), may hold values from 0.3 to 0.8
- head_gain: float32 [128], replicated, may hold values from 0.1 to 1.9
- out_narrow: bfloat16 [1024, 2048], replicated, may hold values from -0.125 to 0.125
- out_wide: bfloat16 [1024, 2048], replicated, may hold values from -0.125 to 0.125
- norm1_gain: float32 [2048], replicated, may hold values from 0.1 to 1.9
- norm2_gain: float32 [2048], replicated, may hold values from 0.1 to 1.9
- expert_ids: int32 [10240, 2], P(('sp', 'tp')), may hold values from 0 to 31, all different within a row; in each aligned block of 40 rows (0 to 39, 40 to 79, ...) at most 3 rows name the same one
- expert_weight: float32 [10240, 2], P(('sp', 'tp')), may hold values from 0.1 to 1
- gate_proj: bfloat16 [32, 2048, 2048], P('sp', None, 'tp'), may hold values from -0.125 to 0.125
- up_proj: bfloat16 [32, 2048, 2048], P('sp', None, 'tp'), may hold values from -0.125 to 0.125
- down_proj: bfloat16 [32, 2048, 2048], P('sp', 'tp'), may hold values from -0.125 to 0.125
Outputs:
- layer_out: bfloat16 [10240, 2048], P(('sp', 'tp'))
The draws below stay inside these ranges and needn't reach their ends.
Inputs may be any that keep to these rules, and one draw needn't show every extreme that they name: `expert_ids`: each row names 2 different experts. Among the 40 rows of one device no expert is named more than 3 times, and in some device's rows some expert is named exactly 3 times.
All inputs are finite; a program needn't handle non-finite values.
Results may differ from the reference program's by a relative error of at most 0.014.
Values may be sent and summed in bfloat16 or wider, within the bound.
A program may use at most 128 MiB of HBM per device.

```python
import math
import jax
import jax.numpy as jnp
import numpy as np
from jax import lax

D = 2048
HG = 8
DKS = 64
DKB = 128
VD = 128
FF = 2048
TOPK = 2
TOK_DEV = 320
TOKENS = 10240
TR = 40
EXPERTS = 32
CAP = 3
N_TP = 8


def drawn_pair(key, key_size):
    width = HG * 2 * key_size
    key_query, key_keys = jax.random.split(key, 2)
    query = jnp.clip(1.3 * jax.random.normal(key_query, (TOKENS, width), jnp.float32), -5.2, 5.2)
    keys = jnp.clip(1.3 * jax.random.normal(key_keys, (TOKENS, width), jnp.float32), -5.2, 5.2)
    return (query, keys)


def draw_query_narrow(key, part):
    return drawn_pair(jax.random.fold_in(key, 11), DKS)[0].astype(jnp.bfloat16)


def draw_key_narrow(key, part):
    return drawn_pair(jax.random.fold_in(key, 11), DKS)[1].astype(jnp.bfloat16)


def draw_query_wide(key, part):
    return drawn_pair(jax.random.fold_in(key, 12), DKB)[0].astype(jnp.bfloat16)


def draw_key_wide(key, part):
    return drawn_pair(jax.random.fold_in(key, 12), DKB)[1].astype(jnp.bfloat16)


def shard_levels(key, dims, cuts, least, largest):
    def one(dim, parts):
        draws = jax.random.uniform(jax.random.fold_in(jax.random.fold_in(key, 6), dim), (parts,), jnp.float32, least / len(cuts), largest / len(cuts))
        return jnp.repeat(jnp.exp(draws), dims[dim] // parts).reshape((-1,) + (1,) * (len(dims) - dim - 1))

    loudness = one(*cuts[0])
    for cut in cuts[1:]:
        loudness = loudness * one(*cut)
    return loudness


def routed_block(stream_key, own, number, rows, amount, top, limit, slope):
    order = jax.random.permutation(stream_key, amount)
    crowded, ordinary = portions_of(amount, rows * top, limit, slope, True), portions_of(amount, rows * top, limit, slope, False)
    places = jnp.arange(amount)

    def named(sizes, rotation):
        used = int((sizes > 0).sum())
        fixed = max(1, used // 4)
        passed = fixed + (places - fixed + rotation * (used - fixed)) % max(1, amount - fixed)
        return jnp.zeros((amount,), jnp.int32).at[order[jnp.where(places < fixed, places, passed)]].set(jnp.asarray(sizes, jnp.int32))

    sizes = jnp.where(number % 4 == 0, named(crowded, number // 4), named(ordinary, number - number // 4 - 1))
    mixed = jax.random.permutation(jax.random.fold_in(own, 3), amount)
    giver, sink = mixed[0:amount // 2 * 2:2], mixed[1:amount // 2 * 2:2]
    room = jnp.minimum(sizes[giver] - 1, limit - sizes[sink]) // 2
    room = jnp.where((giver == order[0]) | (sink == order[0]) | (sizes[sink] == 0), 0, jnp.maximum(room, 0))
    passed = jax.random.randint(jax.random.fold_in(own, 4), (amount // 2,), 0, 1 << 20) % (room + 1)
    sizes = sizes.at[giver].add(-passed).at[sink].add(passed)
    items = jnp.searchsorted(jnp.cumsum(sizes), jnp.arange(rows * top), side="right").astype(jnp.int32)
    grid = items.reshape(top, rows).T
    grid = grid[jax.random.permutation(jax.random.fold_in(own, 1), rows)]
    rotation = jax.random.randint(jax.random.fold_in(own, 2), (rows, 1), 0, top)
    return jnp.take_along_axis(grid, (jnp.arange(top)[None, :] + rotation) % top, axis=1)


def portions_of(number_of, total, reach, skew, full):
    portions = [(1 << 20) // math.isqrt(rank ** skew) + 1 for rank in range(1, number_of + 1)]
    largest = reach if full else min(reach, max(-(-total // number_of), total * portions[0] // sum(portions)))
    least = 1 if total - largest >= number_of - 1 else 0
    given, rest = [largest] + [least] * (number_of - 1), total - largest - least * (number_of - 1)
    while rest > 0:
        candidates = [i for i in range(1, number_of) if given[i] < largest] or [i for i in range(1, number_of) if given[i] < reach]
        whole, left = sum([portions[i] for i in candidates]), rest
        for i in candidates:
            more = min(reach - given[i], max(1, left * portions[i] // whole), rest)
            given[i] = given[i] + more
            rest = rest - more
    return np.array(given)


def gaussian(rng, extent, scale, bound, shards=(), kind=jnp.bfloat16):
    result = scale * jax.random.normal(rng, extent, jnp.float32)
    if shards:
        result = result * shard_levels(rng, extent, shards, -0.22, 0.18)
    return jnp.clip(result, -bound, bound).astype(kind)


def setup_inputs(seed: int = 0) -> dict:
    seeds = jax.random.split(jax.random.key(seed), 20)
    residual = gaussian(seeds[0], (TOKENS, D), 1.0, 6.0, ((0, 256),))
    query_narrow = draw_query_narrow(jax.random.fold_in(seeds[19], 71), 0)
    key_narrow = draw_key_narrow(jax.random.fold_in(seeds[19], 71), 0)
    value_narrow = gaussian(seeds[3], (TOKENS, HG * VD), 1.0, 6.0, ((0, 32), (1, 8)))
    query_wide = draw_query_wide(jax.random.fold_in(seeds[19], 71), 0)
    key_wide = draw_key_wide(jax.random.fold_in(seeds[19], 71), 0)
    value_wide = gaussian(seeds[6], (TOKENS, HG * VD), 1.0, 6.0, ((0, 32), (1, 8)))
    subtract_narrow = jnp.clip(0.3 + 0.5 * jax.random.uniform(seeds[7], (HG,), jnp.float32) ** shard_levels(seeds[7], (HG,), ((0, 8),), -0.2, 0.2), 0.3, 0.8)
    subtract_wide = jnp.clip(0.3 + 0.5 * jax.random.uniform(seeds[8], (HG,), jnp.float32) ** shard_levels(seeds[8], (HG,), ((0, 8),), -0.2, 0.2), 0.3, 0.8)
    head_gain = jnp.clip(1.0 + 0.18 * jax.random.normal(seeds[9], (VD,), jnp.float32), 0.1, 1.9)
    out_narrow = gaussian(seeds[10], (HG * VD, D), (2 * HG * VD) ** -0.5, 0.125)
    out_wide = gaussian(seeds[11], (HG * VD, D), (2 * HG * VD) ** -0.5, 0.125)
    norm1_gain = jnp.clip(1.0 + 0.18 * jax.random.normal(seeds[12], (D,), jnp.float32), 0.1, 1.9)
    norm2_gain = jnp.clip(1.0 + 0.18 * jax.random.normal(seeds[13], (D,), jnp.float32), 0.1, 1.9)
    expert_ids_keys = jax.random.split(jax.random.fold_in(seeds[14], 1), TOKENS // TR)
    expert_ids_turns = jax.random.permutation(jax.random.fold_in(seeds[14], 3), TOKENS // TR)
    expert_ids = jax.vmap(lambda own, number: routed_block(jax.random.fold_in(seeds[14], 2), own, number, TR, EXPERTS, TOPK, CAP, 2))(expert_ids_keys, expert_ids_turns).reshape((TOKENS, TOPK))
    expert_weight = jnp.clip(0.1 + 0.9 * jax.random.uniform(seeds[15], (TOKENS, TOPK), jnp.float32) ** shard_levels(seeds[15], (TOKENS, TOPK), ((0, 256),), -0.2, 0.2), 0.1, 1.0)
    gate_proj = gaussian(seeds[16], (EXPERTS, D, FF), D ** -0.5, 0.125, ((0, 32), (2, 8)))
    up_proj = gaussian(seeds[17], (EXPERTS, D, FF), D ** -0.5, 0.125, ((0, 32), (2, 8)))
    down_proj = gaussian(seeds[18], (EXPERTS, FF, D), FF ** -0.5, 0.125, ((0, 32), (1, 8)))
    return {"residual": residual, "query_narrow": query_narrow, "key_narrow": key_narrow, "value_narrow": value_narrow, "query_wide": query_wide, "key_wide": key_wide, "value_wide": value_wide, "subtract_narrow": subtract_narrow, "subtract_wide": subtract_wide, "head_gain": head_gain, "out_narrow": out_narrow, "out_wide": out_wide, "norm1_gain": norm1_gain, "norm2_gain": norm2_gain, "expert_ids": expert_ids, "expert_weight": expert_weight, "gate_proj": gate_proj, "up_proj": up_proj, "down_proj": down_proj}


residual_scale = 2.0 ** 0.5

def layer_norm(values, gain):
    center = lax.optimization_barrier(jnp.mean(values, -1, keepdims=True))
    spread = lax.optimization_barrier(jnp.mean(jnp.square(values - center), -1, keepdims=True))
    return (values - center) * lax.rsqrt(spread + 1e-05) * gain

def attend_block(block, keys, values, subtract, head_gain, key_size):
    scores = jnp.einsum('qhmd,khmd->hmqk', block.astype(jnp.float32), keys.astype(jnp.float32)) * key_size ** (-0.5)
    rowtop = lax.optimization_barrier(jnp.max(scores, -1, keepdims=True))
    expo = jnp.exp(scores - rowtop)
    total = lax.optimization_barrier(jnp.sum(expo, -1))
    weights = expo.astype(jnp.bfloat16)
    mapped = jnp.einsum('hmqk,khe->hmqe', weights.astype(jnp.float32), values.astype(jnp.float32)) / total[..., None]
    diff = mapped[:, 0] - subtract[:, None, None] * mapped[:, 1]
    normed = diff * lax.rsqrt(lax.optimization_barrier(jnp.mean(diff * diff, -1, keepdims=True)) + 1e-06) * head_gain
    return jnp.transpose(normed, (1, 0, 2)).reshape(block.shape[0], -1).astype(jnp.bfloat16)

def attend(query, keys, values, subtract, head_gain):
    tokens = query.shape[0]
    head_count = subtract.shape[0]
    key_size = query.shape[1] // (2 * head_count)
    queries = query.reshape(tokens, head_count, 2, key_size)
    key_rows = keys.reshape(tokens, head_count, 2, key_size)
    value_rows = values.reshape(tokens, head_count, -1)
    span = math.gcd(tokens, 256)
    blocks = queries.reshape(tokens // span, span, head_count, 2, key_size)

    def one_block(block):
        return attend_block(block, key_rows, value_rows, subtract, head_gain, key_size)
    return lax.map(one_block, blocks).reshape(tokens, -1)

def experts_output(hidden, expert_ids, expert_weight, gate_proj, up_proj, down_proj):
    tokens, top_count = expert_ids.shape
    experts = gate_proj.shape[0]
    rows = TOK_DEV // N_TP
    blocks = tokens // rows
    capacity = max(2, 3 * rows * top_count // (2 * experts))
    ids = expert_ids.reshape(blocks, rows * top_count)
    onehot = (ids[..., None] == jnp.arange(experts, dtype=jnp.int32)).astype(jnp.int32)
    before = jnp.cumsum(onehot, 1) - onehot
    position = lax.optimization_barrier(jnp.sum(before * onehot, -1)).astype(jnp.int32)
    column = jnp.arange(blocks, dtype=jnp.int32)[:, None] * capacity + position
    owner = jnp.repeat(jnp.arange(tokens, dtype=jnp.int32), top_count).reshape(blocks, rows * top_count)
    table = jnp.full((experts, blocks * capacity), tokens, jnp.int32)
    table = table.at[ids.reshape(-1), column.reshape(-1)].set(owner.reshape(-1))
    padded = jnp.concatenate([hidden, jnp.zeros((1, hidden.shape[1]), jnp.bfloat16)], 0)
    width = gate_proj.shape[2] // N_TP

    def one_expert(operands):
        picks, w_gate, w_up, w_down = operands
        taken = padded[picks]
        summed = jnp.zeros((picks.shape[0], hidden.shape[1]), jnp.float32)
        for piece in range(N_TP):
            gate_part = jnp.dot(taken, w_gate[:, piece * width:(piece + 1) * width], preferred_element_type=jnp.float32)
            up_part = jnp.dot(taken, w_up[:, piece * width:(piece + 1) * width], preferred_element_type=jnp.float32)
            inner = (jax.nn.silu(gate_part) * up_part).astype(jnp.bfloat16)
            partial_out = jnp.dot(inner, w_down[piece * width:(piece + 1) * width], preferred_element_type=jnp.float32)
            rounded = lax.optimization_barrier(partial_out.astype(jnp.bfloat16))
            summed = summed + rounded.astype(jnp.float32)
        return summed.astype(jnp.bfloat16)
    results = lax.map(one_expert, (table, gate_proj, up_proj, down_proj))
    flat = results.reshape(experts * blocks * capacity, -1)
    where_rows = (ids * (blocks * capacity) + column).reshape(tokens, top_count)
    gathered = flat[where_rows].astype(jnp.float32)
    return lax.optimization_barrier(jnp.sum(expert_weight[..., None] * gathered, 1))

def reference(residual, query_narrow, key_narrow, value_narrow, query_wide, key_wide, value_wide, subtract_narrow, subtract_wide, head_gain, out_narrow, out_wide, norm1_gain, norm2_gain, expert_ids, expert_weight, gate_proj, up_proj, down_proj):
    attended_narrow = attend(query_narrow, key_narrow, value_narrow, subtract_narrow, head_gain)
    attended_wide = attend(query_wide, key_wide, value_wide, subtract_wide, head_gain)
    mix = jnp.dot(attended_narrow, out_narrow, preferred_element_type=jnp.float32) + jnp.dot(attended_wide, out_wide, preferred_element_type=jnp.float32)
    hidden = layer_norm(residual_scale * residual.astype(jnp.float32) + mix, norm1_gain).astype(jnp.bfloat16)
    routed = experts_output(hidden, expert_ids, expert_weight, gate_proj, up_proj, down_proj)
    return layer_norm(residual_scale * hidden.astype(jnp.float32) + routed, norm2_gain).astype(jnp.bfloat16)
```

```python
import functools

import jax
import jax.numpy as jnp
from jax import lax
from jax.experimental import pallas as pl
from jax.experimental.pallas import tpu as pltpu
from jax.sharding import PartitionSpec as P

residual_scale = 2.0**0.5
MESH = pl.DeviceIdType.MESH


def items_in_groups(value, axis, split_dim, concat_dim, work, item_dim, out_dim):
    items = jax.tree.leaves(value)[0].shape[item_dim]
    count = 2 if items % 2 == 0 else 1
    outs = []
    for k in range(count):
        group = jax.tree.map(
            lambda a: lax.slice_in_dim(
                a, k * (items // count), (k + 1) * (items // count), axis=item_dim
            ),
            value,
        )
        outs.append(
            work(
                lax.all_to_all(
                    group, axis, split_axis=split_dim, concat_axis=concat_dim, tiled=True
                )
            )
        )
    return jax.tree.map(lambda *parts: jnp.concatenate(parts, axis=out_dim), *outs)


def layer_norm(values, gain):
    center = jnp.mean(values, -1, keepdims=True)
    spread = jnp.mean(jnp.square(values - center), -1, keepdims=True)
    return (values - center) * lax.rsqrt(spread + 1e-05) * gain


LOG2E = 1.4426950408889634
Z_RING = 8
X_RING = 4
NARROW = (128, 384)
WIDE = (384, 768)
ROW = 896
PLACE = (0, 1, 3, 5, 7, 6, 4, 2)
QPLACE = (3, 1, 0, 2)


def attend_kernel(
    tok,
    query_narrow,
    key_narrow,
    value_narrow,
    query_wide,
    key_wide,
    value_wide,
    subtract,
    head_gain,
    out,
    queries,
    keys,
    top,
    acc,
    stats,
    share,
    share_stats,
    got,
    got_stats,
    attended,
    gathered,
    local_sem,
    q_send,
    q_recv,
    kv_send,
    kv_recv,
    o_send,
    o_recv,
    s_send,
    s_recv,
    a_send,
    a_recv,
):
    sp = lax.axis_index("sp")
    tp = lax.axis_index("tp")
    heads = lax.axis_size("tp")
    z, x = sp // X_RING, sp % X_RING

    def along_z(k):
        return (lax.rem(z + k, Z_RING) * X_RING + x, tp)

    def along_x(k):
        return (z * X_RING + lax.rem(x + k, X_RING), tp)

    def along_tp(k):
        return (sp, lax.rem(tp + k, heads))

    own_q = QPLACE[0] * tok
    loads = [
        pltpu.make_async_copy(src, dst, local_sem.at[i])
        for i, (src, dst) in enumerate(
            (
                (query_narrow, queries.at[pl.ds(own_q, tok), pl.ds(0, 128)]),
                (query_wide, queries.at[pl.ds(own_q, tok), pl.ds(128, 256)]),
                (value_narrow, keys.at[pl.ds(0, tok), pl.ds(128, 128)]),
                (key_narrow, keys.at[pl.ds(0, tok), pl.ds(256, 128)]),
                (key_wide, keys.at[pl.ds(0, tok), pl.ds(384, 256)]),
                (value_wide, keys.at[pl.ds(0, tok), pl.ds(640, 128)]),
            )
        )
    ]
    for c in loads:
        c.start()

    barrier = pltpu.get_barrier_semaphore()
    peers = (
        [along_z(1), along_z(Z_RING - 1)]
        + [along_x(k) for k in range(1, X_RING)]
        + [along_tp(k) for k in range(1, heads)]
    )
    for peer in peers:
        pl.semaphore_signal(barrier, inc=1, device_id=peer, device_id_type=MESH)
    keys[:, 0:128] = jnp.ones((keys.shape[0], 128), jnp.bfloat16)
    keys[:, 768:896] = jnp.ones((keys.shape[0], 128), jnp.bfloat16)
    top[...] = jnp.full(top.shape, -1e30, jnp.float32)
    acc[...] = jnp.zeros(acc.shape, jnp.float32)
    stats[...] = jnp.zeros(stats.shape, jnp.float32)
    for c in loads:
        c.wait()
    pl.semaphore_wait(barrier, len(peers))

    def remote(src, dst, send, recv, peer):
        return pltpu.make_async_remote_copy(
            src_ref=src, dst_ref=dst, send_sem=send, recv_sem=recv, device_id=peer,
            device_id_type=MESH,
        )

    def ring_copy(way, step, piece):
        cols = WIDE if piece else NARROW
        forward = way == 0
        source = (Z_RING - step + 1) % Z_RING if forward else step - 1
        target = (Z_RING - step) % Z_RING if forward else step
        r0, rows = 0, tok
        if 2 * step == Z_RING:
            rows = tok // 2
            r0 = 0 if forward else rows
        at = lambda k: keys.at[
            pl.ds(PLACE[k] * tok + r0, rows), pl.ds(cols[0], cols[1] - cols[0])
        ]
        n = (way * (Z_RING // 2) + step - 1) * 2 + piece
        return remote(
            at(source), at(target), kv_send.at[n], kv_recv.at[n],
            along_z(1 if forward else Z_RING - 1),
        )

    def query_copy(k):
        return remote(
            queries.at[pl.ds(own_q, tok), :],
            queries.at[pl.ds(QPLACE[(X_RING - k) % X_RING] * tok, tok), :],
            q_send.at[k], q_recv.at[k], along_x(k),
        )

    ring = {
        (w, s, p): ring_copy(w, s, p)
        for w in range(2)
        for s in range(1, Z_RING // 2 + 1)
        for p in range(2)
    }
    query_copies = {k: query_copy(k) for k in range(1, X_RING)}

    def start_step(step, piece):
        for w in range(2):
            ring[w, step, piece].start()

    def arrived(step, piece):
        for w in range(2):
            ring[w, step, piece].wait_recv()

    start_step(1, 0)
    for k in (1, 3, 2):
        query_copies[k].start()
    start_step(1, 1)

    pair = 2 * tok

    def absorb(head, group, k0, span):
        rows = pl.ds(k0, span)
        qrows = pl.ds(group * pair, pair)
        size = 128 if head else 64
        scale = size**-0.5 * LOG2E
        scores = []
        for m in range(2):
            if head:
                q = queries[qrows, 128 + 128 * m : 256 + 128 * m]
                k = keys[rows, 384 + 128 * m : 512 + 128 * m]
            else:
                q = queries[qrows, 0:128]
                lane = lax.broadcasted_iota(jnp.int32, q.shape, 1)
                q = jnp.where((lane < 64) if m == 0 else (lane >= 64), q, jnp.zeros_like(q))
                k = keys[rows, 256:384]
            scores.append(
                lax.dot_general(
                    q, k, (((1,), (1,)), ((), ())), preferred_element_type=jnp.float32
                )
            )
        v = keys[rows, 640:896] if head else keys[rows, 0:256]
        for m in range(2):
            s = scores[m]
            before = top[2 * head + m, qrows, :]
            now = jnp.maximum(before, jnp.max(s, -1, keepdims=True) * scale)
            expo = jnp.exp2(s * scale - now[:, :1])
            shrink = jnp.exp2(before - now)
            add = jnp.dot(expo.astype(jnp.bfloat16), v, preferred_element_type=jnp.float32)
            a = acc[2 * head + m, qrows, :]
            acc[2 * head + m, qrows, :] = (
                jnp.concatenate([a[:, :128] * shrink, a[:, 128:] * shrink], 1) + add
            )
            top[2 * head + m, qrows, :] = now

    def absorb_both(head, k0, span):
        def one(g, carry):
            absorb(head, g, k0, span)
            return carry

        lax.fori_loop(0, 2, one, 0)

    def share_copy(head, k):
        to = (X_RING - k) % X_RING
        n = head * X_RING + k
        return (
            remote(share.at[n], got.at[head * X_RING + to], o_send.at[n], o_recv.at[n], along_x(k)),
            remote(
                share_stats.at[n], got_stats.at[head * X_RING + to], s_send.at[n], s_recv.at[n],
                along_x(k),
            ),
        )

    def finish(head, k):
        n = head * X_RING + k
        qrows = pl.ds(QPLACE[k] * tok, tok)
        lane = lax.broadcasted_iota(jnp.int32, (tok, 128), 1)
        column = jnp.zeros((tok, 128), jnp.float32)
        parts = []
        for m in range(2):
            a = acc[2 * head + m, qrows, :]
            value, total = (a[:, :128], a[:, 128:]) if head else (a[:, 128:], a[:, :128])
            parts.append(value / total)
            column = jnp.where(lane == m, top[2 * head + m, qrows, :] + jnp.log2(total), column)
        both = jnp.concatenate(parts, 1)
        if k == 0:
            got[n] = both.astype(jnp.bfloat16)
        else:
            share[n] = both.astype(jnp.bfloat16)
        stats[0:tok, :] = column
        flat = jnp.transpose(stats[...])[0:8]
        if k == 0:
            got_stats[n] = flat
        else:
            share_stats[n] = flat
            for c in share_copy(head, k):
                c.start()

    def combine(head):
        base = head * X_RING
        for k in range(1, X_RING):
            for c in share_copy(head, k):
                c.wait_recv()
        lse = [got_stats[base + k] for k in range(X_RING)]
        peak = functools.reduce(jnp.maximum, lse)
        weight = [jnp.exp2(v - peak) for v in lse]
        row = lax.broadcasted_iota(jnp.int32, peak.shape, 0)
        factor = jnp.where(row == 1, -subtract[head], 1.0) / functools.reduce(jnp.add, weight)
        wide = jnp.concatenate(
            [w * factor for w in weight]
            + [jnp.zeros((128 - 8 * X_RING, peak.shape[1]), jnp.float32)],
            0,
        )
        turned = jnp.transpose(wide)[0:tok]
        diff = jnp.zeros((tok, 128), jnp.float32)
        for k in range(X_RING):
            o = got[base + k].astype(jnp.float32)
            for m in range(2):
                diff = diff + turned[:, 8 * k + m : 8 * k + m + 1] * o[:, 128 * m : 128 * m + 128]
        spread = jnp.mean(diff * diff, -1, keepdims=True)
        normed = diff * lax.rsqrt(spread + 1e-06) * head_gain[...]
        attended[:, :, 128 * head : 128 * head + 128] = normed.reshape(
            heads, tok // heads, 128
        ).astype(jnp.bfloat16)

    arrived(1, 0)
    start_step(2, 0)
    query_copies[1].wait_recv()
    absorb(0, 1, 0, 256)
    absorb(1, 1, 0, 256)
    query_copies[3].wait_recv()
    query_copies[2].wait_recv()
    absorb(0, 0, 0, 256)
    absorb(1, 0, 0, 256)
    arrived(1, 1)
    start_step(2, 1)
    absorb_both(0, 256, 512)
    absorb_both(1, 256, 512)
    arrived(2, 0)
    start_step(3, 0)
    absorb_both(0, 768, 768)
    arrived(2, 1)
    start_step(3, 1)
    absorb_both(1, 768, 768)
    arrived(3, 0)
    start_step(4, 0)
    absorb_both(0, 1536, 512)
    arrived(3, 1)
    start_step(4, 1)
    absorb_both(1, 1536, 512)
    for head in range(2):
        arrived(4, head)
        absorb(head, 0, 2048, 512)
        finish(head, 2)
        finish(head, 1)
        absorb(head, 1, 2048, 512)
        finish(head, 3)
        finish(head, 0)
    for head in range(2):
        combine(head)

    def head_copy(k):
        return remote(
            attended.at[lax.rem(tp + k, heads)], gathered.at[tp], a_send.at[k], a_recv.at[k],
            along_tp(k),
        )

    for k in range(1, heads):
        head_copy(k).start()
    gathered[pl.ds(tp, 1)] = attended[pl.ds(tp, 1)]
    for k in range(1, heads):
        head_copy(k).wait_recv()
    out[...] = gathered[...]
    for c in ring.values():
        c.wait_send()
    for c in query_copies.values():
        c.wait_send()
    for head in range(2):
        for k in range(1, X_RING):
            for c in share_copy(head, k):
                c.wait_send()
    for k in range(1, heads):
        head_copy(k).wait_send()


def attend(
    query_narrow, key_narrow, value_narrow, query_wide, key_wide, value_wide, subtract_narrow,
    subtract_wide, head_gain,
):
    tok = query_narrow.shape[0]
    heads = lax.axis_size("tp")
    lanes = (tok + 127) // 128 * 128
    vmem = pl.BlockSpec(memory_space=pltpu.VMEM)
    hbm = pl.BlockSpec(memory_space=pl.ANY)
    dma = pltpu.SemaphoreType.DMA
    bf16, f32 = jnp.bfloat16, jnp.float32
    return pl.pallas_call(
        functools.partial(attend_kernel, tok),
        out_shape=jax.ShapeDtypeStruct((heads, tok // heads, 256), bf16),
        in_specs=[hbm] * 6 + [pl.BlockSpec(memory_space=pltpu.SMEM), vmem],
        out_specs=vmem,
        scratch_shapes=[
            pltpu.VMEM((X_RING * tok, 384), bf16),
            pltpu.VMEM((Z_RING * tok, ROW), bf16),
            pltpu.VMEM((4, X_RING * tok, 128), f32),
            pltpu.VMEM((4, X_RING * tok, 256), f32),
            pltpu.VMEM((lanes, 128), f32),
            pltpu.VMEM((2 * X_RING, tok, 256), bf16),
            pltpu.VMEM((2 * X_RING, 8, lanes), f32),
            pltpu.VMEM((2 * X_RING, tok, 256), bf16),
            pltpu.VMEM((2 * X_RING, 8, lanes), f32),
            pltpu.VMEM((heads, tok // heads, 256), bf16),
            pltpu.VMEM((heads, tok // heads, 256), bf16),
            dma((6,)),
            dma((X_RING,)),
            dma((X_RING,)),
            dma((2 * Z_RING,)),
            dma((2 * Z_RING,)),
            dma((2 * X_RING,)),
            dma((2 * X_RING,)),
            dma((2 * X_RING,)),
            dma((2 * X_RING,)),
            dma((heads,)),
            dma((heads,)),
        ],
        compiler_params=pltpu.CompilerParams(
            collective_id=0, has_side_effects=True, vmem_limit_bytes=56 * 1024 * 1024
        ),
        name="attend",
    )(
        query_narrow, key_narrow, value_narrow, query_wide, key_wide, value_wide,
        jnp.concatenate([subtract_narrow, subtract_wide]), head_gain.reshape(1, -1),
    )


def mixed_heads(attended, out_narrow, out_wide):
    rows = attended.shape[1]
    turned = jnp.transpose(attended, (1, 0, 2))
    narrow = turned[:, :, :128].reshape(rows, -1)
    wide = turned[:, :, 128:].reshape(rows, -1)
    return jnp.dot(narrow, out_narrow, preferred_element_type=jnp.float32) + jnp.dot(
        wide, out_wide, preferred_element_type=jnp.float32
    )


def on_device(
    residual,
    query_narrow,
    key_narrow,
    value_narrow,
    query_wide,
    key_wide,
    value_wide,
    subtract_narrow,
    subtract_wide,
    head_gain,
    out_narrow,
    out_wide,
    norm1_gain,
    norm2_gain,
    expert_ids,
    expert_weight,
    gate_proj,
    up_proj,
    down_proj,
):
    attended = attend(
        query_narrow, key_narrow, value_narrow, query_wide, key_wide, value_wide,
        subtract_narrow, subtract_wide, head_gain,
    )
    mix = mixed_heads(attended, out_narrow, out_wide)
    hidden = layer_norm(residual_scale * residual.astype(jnp.float32) + mix, norm1_gain).astype(
        jnp.bfloat16
    )
    local_rows, top_count = expert_ids.shape
    experts = lax.axis_size("sp")
    capacity = max(2, 3 * local_rows * top_count // (2 * experts))
    flat_ids = expert_ids.reshape(-1)
    onehot = (flat_ids[:, None] == jnp.arange(experts, dtype=jnp.int32)[None, :]).astype(jnp.int32)
    before = jnp.cumsum(onehot, 0) - onehot
    position = jnp.sum(before * onehot, 1)
    slots = (flat_ids * capacity + position).reshape(local_rows, top_count)
    dispatch_table = jnp.any(
        jnp.arange(experts * capacity, dtype=jnp.int32)[:, None, None] == slots[None], -1
    ).astype(jnp.bfloat16)
    outgoing = jnp.dot(dispatch_table, hidden, preferred_element_type=jnp.float32).astype(
        jnp.bfloat16
    )
    outgoing = outgoing.reshape(experts, capacity, -1)

    def run_expert(received):
        gathered = lax.all_gather(received, "tp", axis=1, tiled=True)
        flat_rows = gathered.reshape(-1, gathered.shape[2])
        gate_part = jnp.dot(flat_rows, gate_proj[0], preferred_element_type=jnp.float32)
        up_part = jnp.dot(flat_rows, up_proj[0], preferred_element_type=jnp.float32)
        inner = (jax.nn.silu(gate_part) * up_part).astype(jnp.bfloat16)
        partial_out = jnp.dot(inner, down_proj[0], preferred_element_type=jnp.float32).reshape(
            gathered.shape
        )
        summed = lax.psum_scatter(
            partial_out.astype(jnp.bfloat16), "tp", scatter_dimension=1, tiled=True
        )
        return lax.all_to_all(summed, "sp", split_axis=0, concat_axis=0, tiled=True)

    returned = items_in_groups(outgoing, "sp", 0, 0, run_expert, 1, 1)
    returned_flat = returned.reshape(experts * capacity, -1)
    picked = returned_flat[slots].astype(jnp.float32)
    routed = jnp.sum(expert_weight[..., None] * picked, 1)
    return layer_norm(residual_scale * hidden.astype(jnp.float32) + routed, norm2_gain).astype(
        jnp.bfloat16
    )


def solution(mesh):
    placed = (
        P(("sp", "tp"), None),
        P("sp", "tp"),
        P("sp", "tp"),
        P("sp", "tp"),
        P("sp", "tp"),
        P("sp", "tp"),
        P("sp", "tp"),
        P("tp"),
        P("tp"),
        P(),
        P(),
        P(),
        P(),
        P(),
        P(("sp", "tp"), None),
        P(("sp", "tp"), None),
        P("sp", None, "tp"),
        P("sp", None, "tp"),
        P("sp", "tp", None),
    )
    return jax.shard_map(
        on_device, mesh=mesh, in_specs=placed, out_specs=P(("sp", "tp"), None), check_vma=False
    )
```

```python
import functools

import jax
import jax.numpy as jnp
from jax import lax
from jax.experimental import pallas as pl
from jax.experimental.pallas import tpu as pltpu
from jax.sharding import PartitionSpec as P

residual_scale = 2.0**0.5
MESH = pl.DeviceIdType.MESH


def layer_norm(values, gain):
    center = jnp.mean(values, -1, keepdims=True)
    spread = jnp.mean(jnp.square(values - center), -1, keepdims=True)
    return (values - center) * lax.rsqrt(spread + 1e-05) * gain


LOG2E = 1.4426950408889634
Z_RING = 8
X_RING = 4
NARROW = (128, 384)
WIDE = (384, 768)
ROW = 896
PLACE = (0, 1, 3, 5, 7, 6, 4, 2)
QPLACE = (3, 1, 0, 2)


def attend_kernel(
    tok,
    query_narrow,
    key_narrow,
    value_narrow,
    query_wide,
    key_wide,
    value_wide,
    subtract,
    head_gain,
    out,
    queries,
    keys,
    top,
    acc,
    stats,
    share,
    share_stats,
    got,
    got_stats,
    attended,
    gathered,
    local_sem,
    q_send,
    q_recv,
    kv_send,
    kv_recv,
    o_send,
    o_recv,
    s_send,
    s_recv,
    a_send,
    a_recv,
):
    sp = lax.axis_index("sp")
    tp = lax.axis_index("tp")
    heads = lax.axis_size("tp")
    z, x = sp // X_RING, sp % X_RING

    def along_z(k):
        return (lax.rem(z + k, Z_RING) * X_RING + x, tp)

    def along_x(k):
        return (z * X_RING + lax.rem(x + k, X_RING), tp)

    def along_tp(k):
        return (sp, lax.rem(tp + k, heads))

    own_q = QPLACE[0] * tok
    loads = [
        pltpu.make_async_copy(src, dst, local_sem.at[i])
        for i, (src, dst) in enumerate(
            (
                (query_narrow, queries.at[pl.ds(own_q, tok), pl.ds(0, 128)]),
                (query_wide, queries.at[pl.ds(own_q, tok), pl.ds(128, 256)]),
                (value_narrow, keys.at[pl.ds(0, tok), pl.ds(128, 128)]),
                (key_narrow, keys.at[pl.ds(0, tok), pl.ds(256, 128)]),
                (key_wide, keys.at[pl.ds(0, tok), pl.ds(384, 256)]),
                (value_wide, keys.at[pl.ds(0, tok), pl.ds(640, 128)]),
            )
        )
    ]
    for c in loads:
        c.start()

    barrier = pltpu.get_barrier_semaphore()
    peers = (
        [along_z(1), along_z(Z_RING - 1)]
        + [along_x(k) for k in range(1, X_RING)]
        + [along_tp(k) for k in range(1, heads)]
    )
    for peer in peers:
        pl.semaphore_signal(barrier, inc=1, device_id=peer, device_id_type=MESH)
    keys[:, 0:128] = jnp.ones((keys.shape[0], 128), jnp.bfloat16)
    keys[:, 768:896] = jnp.ones((keys.shape[0], 128), jnp.bfloat16)
    top[...] = jnp.full(top.shape, -1e30, jnp.float32)
    acc[...] = jnp.zeros(acc.shape, jnp.float32)
    stats[...] = jnp.zeros(stats.shape, jnp.float32)
    for c in loads:
        c.wait()
    pl.semaphore_wait(barrier, len(peers))

    def remote(src, dst, send, recv, peer):
        return pltpu.make_async_remote_copy(
            src_ref=src, dst_ref=dst, send_sem=send, recv_sem=recv, device_id=peer,
            device_id_type=MESH,
        )

    def ring_copy(way, step, piece):
        cols = WIDE if piece else NARROW
        forward = way == 0
        source = (Z_RING - step + 1) % Z_RING if forward else step - 1
        target = (Z_RING - step) % Z_RING if forward else step
        r0, rows = 0, tok
        if 2 * step == Z_RING:
            rows = tok // 2
            r0 = 0 if forward else rows
        at = lambda k: keys.at[
            pl.ds(PLACE[k] * tok + r0, rows), pl.ds(cols[0], cols[1] - cols[0])
        ]
        n = (way * (Z_RING // 2) + step - 1) * 2 + piece
        return remote(
            at(source), at(target), kv_send.at[n], kv_recv.at[n],
            along_z(1 if forward else Z_RING - 1),
        )

    def query_copy(k):
        return remote(
            queries.at[pl.ds(own_q, tok), :],
            queries.at[pl.ds(QPLACE[(X_RING - k) % X_RING] * tok, tok), :],
            q_send.at[k], q_recv.at[k], along_x(k),
        )

    ring = {
        (w, s, p): ring_copy(w, s, p)
        for w in range(2)
        for s in range(1, Z_RING // 2 + 1)
        for p in range(2)
    }
    query_copies = {k: query_copy(k) for k in range(1, X_RING)}

    def start_step(step, piece):
        for w in range(2):
            ring[w, step, piece].start()

    def arrived(step, piece):
        for w in range(2):
            ring[w, step, piece].wait_recv()

    start_step(1, 0)
    for k in (1, 3, 2):
        query_copies[k].start()
    start_step(1, 1)

    pair = 2 * tok

    def absorb(head, group, k0, span):
        rows = pl.ds(k0, span)
        qrows = pl.ds(group * pair, pair)
        size = 128 if head else 64
        scale = size**-0.5 * LOG2E
        scores = []
        for m in range(2):
            if head:
                q = queries[qrows, 128 + 128 * m : 256 + 128 * m]
                k = keys[rows, 384 + 128 * m : 512 + 128 * m]
            else:
                q = queries[qrows, 0:128]
                lane = lax.broadcasted_iota(jnp.int32, q.shape, 1)
                q = jnp.where((lane < 64) if m == 0 else (lane >= 64), q, jnp.zeros_like(q))
                k = keys[rows, 256:384]
            scores.append(
                lax.dot_general(
                    q, k, (((1,), (1,)), ((), ())), preferred_element_type=jnp.float32
                )
            )
        v = keys[rows, 640:896] if head else keys[rows, 0:256]
        for m in range(2):
            s = scores[m]
            before = top[2 * head + m, qrows, :]
            now = jnp.maximum(before, jnp.max(s, -1, keepdims=True) * scale)
            expo = jnp.exp2(s * scale - now[:, :1])
            shrink = jnp.exp2(before - now)
            add = jnp.dot(expo.astype(jnp.bfloat16), v, preferred_element_type=jnp.float32)
            a = acc[2 * head + m, qrows, :]
            acc[2 * head + m, qrows, :] = (
                jnp.concatenate([a[:, :128] * shrink, a[:, 128:] * shrink], 1) + add
            )
            top[2 * head + m, qrows, :] = now

    def absorb_both(head, k0, span):
        def one(g, carry):
            absorb(head, g, k0, span)
            return carry

        lax.fori_loop(0, 2, one, 0)

    def share_copy(head, k):
        to = (X_RING - k) % X_RING
        n = head * X_RING + k
        return (
            remote(share.at[n], got.at[head * X_RING + to], o_send.at[n], o_recv.at[n], along_x(k)),
            remote(
                share_stats.at[n], got_stats.at[head * X_RING + to], s_send.at[n], s_recv.at[n],
                along_x(k),
            ),
        )

    def finish(head, k):
        n = head * X_RING + k
        qrows = pl.ds(QPLACE[k] * tok, tok)
        lane = lax.broadcasted_iota(jnp.int32, (tok, 128), 1)
        column = jnp.zeros((tok, 128), jnp.float32)
        parts = []
        for m in range(2):
            a = acc[2 * head + m, qrows, :]
            value, total = (a[:, :128], a[:, 128:]) if head else (a[:, 128:], a[:, :128])
            parts.append(value / total)
            column = jnp.where(lane == m, top[2 * head + m, qrows, :] + jnp.log2(total), column)
        both = jnp.concatenate(parts, 1)
        if k == 0:
            got[n] = both.astype(jnp.bfloat16)
        else:
            share[n] = both.astype(jnp.bfloat16)
        stats[0:tok, :] = column
        flat = jnp.transpose(stats[...])[0:8]
        if k == 0:
            got_stats[n] = flat
        else:
            share_stats[n] = flat
            for c in share_copy(head, k):
                c.start()

    def combine(head):
        base = head * X_RING
        for k in range(1, X_RING):
            for c in share_copy(head, k):
                c.wait_recv()
        lse = [got_stats[base + k] for k in range(X_RING)]
        peak = functools.reduce(jnp.maximum, lse)
        weight = [jnp.exp2(v - peak) for v in lse]
        row = lax.broadcasted_iota(jnp.int32, peak.shape, 0)
        factor = jnp.where(row == 1, -subtract[head], 1.0) / functools.reduce(jnp.add, weight)
        wide = jnp.concatenate(
            [w * factor for w in weight]
            + [jnp.zeros((128 - 8 * X_RING, peak.shape[1]), jnp.float32)],
            0,
        )
        turned = jnp.transpose(wide)[0:tok]
        diff = jnp.zeros((tok, 128), jnp.float32)
        for k in range(X_RING):
            o = got[base + k].astype(jnp.float32)
            for m in range(2):
                diff = diff + turned[:, 8 * k + m : 8 * k + m + 1] * o[:, 128 * m : 128 * m + 128]
        spread = jnp.mean(diff * diff, -1, keepdims=True)
        normed = diff * lax.rsqrt(spread + 1e-06) * head_gain[...]
        attended[:, :, 128 * head : 128 * head + 128] = normed.reshape(
            heads, tok // heads, 128
        ).astype(jnp.bfloat16)

    arrived(1, 0)
    start_step(2, 0)
    query_copies[1].wait_recv()
    absorb(0, 1, 0, 256)
    absorb(1, 1, 0, 256)
    query_copies[3].wait_recv()
    query_copies[2].wait_recv()
    absorb(0, 0, 0, 256)
    absorb(1, 0, 0, 256)
    arrived(1, 1)
    start_step(2, 1)
    absorb_both(0, 256, 512)
    absorb_both(1, 256, 512)
    arrived(2, 0)
    start_step(3, 0)
    absorb_both(0, 768, 768)
    arrived(2, 1)
    start_step(3, 1)
    absorb_both(1, 768, 768)
    arrived(3, 0)
    start_step(4, 0)
    absorb_both(0, 1536, 512)
    arrived(3, 1)
    start_step(4, 1)
    absorb_both(1, 1536, 512)
    for head in range(2):
        arrived(4, head)
        absorb(head, 0, 2048, 512)
        finish(head, 2)
        finish(head, 1)
        absorb(head, 1, 2048, 512)
        finish(head, 3)
        finish(head, 0)
    for head in range(2):
        combine(head)

    def head_copy(k):
        return remote(
            attended.at[lax.rem(tp + k, heads)], gathered.at[tp], a_send.at[k], a_recv.at[k],
            along_tp(k),
        )

    for k in range(1, heads):
        head_copy(k).start()
    gathered[pl.ds(tp, 1)] = attended[pl.ds(tp, 1)]
    for k in range(1, heads):
        head_copy(k).wait_recv()
    out[...] = gathered[...]
    for c in ring.values():
        c.wait_send()
    for c in query_copies.values():
        c.wait_send()
    for head in range(2):
        for k in range(1, X_RING):
            for c in share_copy(head, k):
                c.wait_send()
    for k in range(1, heads):
        head_copy(k).wait_send()


def attend(
    query_narrow, key_narrow, value_narrow, query_wide, key_wide, value_wide, subtract_narrow,
    subtract_wide, head_gain,
):
    tok = query_narrow.shape[0]
    heads = lax.axis_size("tp")
    lanes = (tok + 127) // 128 * 128
    vmem = pl.BlockSpec(memory_space=pltpu.VMEM)
    hbm = pl.BlockSpec(memory_space=pl.ANY)
    dma = pltpu.SemaphoreType.DMA
    bf16, f32 = jnp.bfloat16, jnp.float32
    return pl.pallas_call(
        functools.partial(attend_kernel, tok),
        out_shape=jax.ShapeDtypeStruct((heads, tok // heads, 256), bf16),
        in_specs=[hbm] * 6 + [pl.BlockSpec(memory_space=pltpu.SMEM), vmem],
        out_specs=vmem,
        scratch_shapes=[
            pltpu.VMEM((X_RING * tok, 384), bf16),
            pltpu.VMEM((Z_RING * tok, ROW), bf16),
            pltpu.VMEM((4, X_RING * tok, 128), f32),
            pltpu.VMEM((4, X_RING * tok, 256), f32),
            pltpu.VMEM((lanes, 128), f32),
            pltpu.VMEM((2 * X_RING, tok, 256), bf16),
            pltpu.VMEM((2 * X_RING, 8, lanes), f32),
            pltpu.VMEM((2 * X_RING, tok, 256), bf16),
            pltpu.VMEM((2 * X_RING, 8, lanes), f32),
            pltpu.VMEM((heads, tok // heads, 256), bf16),
            pltpu.VMEM((heads, tok // heads, 256), bf16),
            dma((6,)),
            dma((X_RING,)),
            dma((X_RING,)),
            dma((2 * Z_RING,)),
            dma((2 * Z_RING,)),
            dma((2 * X_RING,)),
            dma((2 * X_RING,)),
            dma((2 * X_RING,)),
            dma((2 * X_RING,)),
            dma((heads,)),
            dma((heads,)),
        ],
        compiler_params=pltpu.CompilerParams(
            collective_id=0, has_side_effects=True, vmem_limit_bytes=56 * 1024 * 1024
        ),
        name="attend",
    )(
        query_narrow, key_narrow, value_narrow, query_wide, key_wide, value_wide,
        jnp.concatenate([subtract_narrow, subtract_wide]), head_gain.reshape(1, -1),
    )


def mixed_heads(attended, out_narrow, out_wide):
    rows = attended.shape[1]
    turned = jnp.transpose(attended, (1, 0, 2))
    narrow = turned[:, :, :128].reshape(rows, -1)
    wide = turned[:, :, 128:].reshape(rows, -1)
    return jnp.dot(narrow, out_narrow, preferred_element_type=jnp.float32) + jnp.dot(
        wide, out_wide, preferred_element_type=jnp.float32
    )


Y_RING = 4
STEPS_Z = (0, 1, 7, 4, 2, 6, 3, 5)
GROUPS = 2
LANES = 128


def to_tiles(values, words, target, first):
    rows, width = values.shape
    tall = width // LANES
    for j in range(tall):
        words[pl.ds(j, rows, stride=tall), :] = values[:, LANES * j : LANES * (j + 1)]
    flat = words[0 : rows * tall, :]
    target[first : first + rows] = flat.reshape(rows, tall, LANES).astype(jnp.bfloat16)


def from_tiles(source, first, rows, words, target):
    tall = source.shape[1]
    flat = source[first : first + rows].astype(jnp.float32)
    words[0 : rows * tall, :] = flat.reshape(rows * tall, LANES)
    for j in range(tall):
        target[:, LANES * j : LANES * (j + 1)] = words[pl.ds(j, rows, stride=tall), :].astype(
            jnp.bfloat16
        )


def experts_kernel(
    capacity,
    hidden,
    slots_across,
    slots_down,
    expert_weight,
    norm2_gain,
    gate_proj,
    up_proj,
    down_proj,
    out,
    gate,
    up,
    down,
    words,
    outgoing,
    received,
    gathered,
    partial,
    from_core,
    half_sum,
    from_half,
    whole_sum,
    from_side,
    results,
    returned,
    returned_rows,
    w_sem,
    d_send,
    d_recv,
    g_send,
    g_recv,
    c_send,
    c_recv,
    h_send,
    h_recv,
    f_send,
    f_recv,
    r_send,
    r_recv,
):
    sp = lax.axis_index("sp")
    tp = lax.axis_index("tp")
    z, x = sp // X_RING, sp % X_RING
    y, core = tp // 2, tp % 2
    experts = Z_RING * X_RING
    width = hidden.shape[1]
    half = width // 2
    f32, bf16 = jnp.float32, jnp.bfloat16

    def expert_at(dz, dx):
        return lax.rem(z + dz, Z_RING) * X_RING + lax.rem(x + dx, X_RING)

    def along_y(k):
        return (sp, lax.rem(y + k, Y_RING) * 2 + core)

    sibling = (sp, y * 2 + 1 - core)
    loads = [
        pltpu.make_async_copy(src.at[0], dst, w_sem.at[i])
        for i, (src, dst) in enumerate(((gate_proj, gate), (up_proj, up), (down_proj, down)))
    ]
    for c in loads:
        c.start()
    others = [(dz, dx) for dz in STEPS_Z for dx in range(X_RING) if dz or dx]
    peers = [(expert_at(dz, dx), tp) for dz, dx in others]
    peers = peers + [sibling, along_y(1), along_y(Y_RING - 1)]
    barrier = pltpu.get_barrier_semaphore()
    for peer in peers:
        pl.semaphore_signal(barrier, inc=1, device_id=peer, device_id_type=MESH)

    local_rows, top_count = expert_weight.shape
    row = lax.broadcasted_iota(jnp.int32, (experts * capacity, local_rows), 0)
    table = jnp.zeros(row.shape, f32)
    for c in range(top_count):
        table = jnp.where(row == slots_across[c : c + 1, :], 1.0, table)
    rows = jnp.dot(table.astype(bf16), hidden[...], preferred_element_type=f32)
    to_tiles(rows, words, outgoing, 0)
    pl.semaphore_wait(barrier, len(peers))

    def remote(src, dst, send, recv, peer):
        return pltpu.make_async_remote_copy(
            src_ref=src, dst_ref=dst, send_sem=send, recv_sem=recv, device_id=peer,
            device_id_type=MESH,
        )

    def place(dz, dx):
        return STEPS_Z.index(dz % Z_RING) * X_RING + dx % X_RING

    def dispatch_copy(dz, dx):
        e = expert_at(dz, dx)
        p = place(-dz, -dx)
        return remote(
            outgoing.at[pl.ds(e * capacity, capacity)],
            received.at[pl.ds(p * capacity, capacity)],
            d_send.at[p], d_recv.at[p], (e, tp),
        )

    def return_copy(dz, dx):
        p = place(dz, dx)
        return remote(
            results.at[pl.ds(p * capacity, capacity)],
            returned.at[pl.ds(sp * capacity, capacity)],
            r_send.at[p], r_recv.at[p], (expert_at(dz, dx), tp),
        )

    per_group = len(STEPS_Z) // GROUPS
    steps_of = [STEPS_Z[g * per_group : (g + 1) * per_group] for g in range(GROUPS)]
    hops = [[(dz, dx) for dz in steps_of[g] for dx in range(X_RING)] for g in range(GROUPS)]
    block = per_group * X_RING * capacity
    low, high = pl.ds(0, half), pl.ds(half, half)

    for g in range(GROUPS):
        for dz, dx in hops[g]:
            if dz or dx:
                dispatch_copy(dz, dx).start()

    def gather_copies(g):
        at = lambda s, c=None: gathered.at[g, s] if c is None else gathered.at[g, s, :, c]
        right, left = along_y(1), along_y(Y_RING - 1)
        plan = {
            "core0": (at(0), at(1), sibling),
            "right": (at(0), at(6), right),
            "left": (at(0), at(2), left),
            "right2": (at(6, low), at(4, low), right),
            "left2": (at(2, high), at(4, high), left),
            "core1": (at(2), at(3), sibling),
            "core3": (at(6), at(7), sibling),
            "core2": (at(4), at(5), sibling),
        }
        return {
            name: remote(src, dst, g_send.at[g, i], g_recv.at[g, i], peer)
            for i, (name, (src, dst, peer)) in enumerate(plan.items())
        }

    gathers = [gather_copies(g) for g in range(GROUPS)]

    def core_copy(g, k):
        return remote(
            partial.at[g, 2 * k + 1], from_core.at[g, k], c_send.at[g, k], c_recv.at[g, k], sibling
        )

    def half_copy(g, way):
        return remote(
            half_sum.at[g, way], from_half.at[g, way], h_send.at[g, way], h_recv.at[g, way],
            along_y(Y_RING - 1 if way else 1),
        )

    def side_copy(g, way, part):
        cols = high if part else low
        return remote(
            whole_sum.at[g, way, :, cols], from_side.at[g, way, :, cols],
            f_send.at[g, way, part], f_recv.at[g, way, part], along_y(Y_RING - 1 if way else 1),
        )

    def open_group(g):
        for dz, dx in hops[g]:
            p = place(dz, dx)
            if dz or dx:
                dispatch_copy(-dz % Z_RING, -dx % X_RING).wait_recv()
            else:
                received[p * capacity : (p + 1) * capacity] = outgoing[
                    pl.ds(sp * capacity, capacity)
                ]
        from_tiles(received, g * block, block, words, gathered.at[g, 0])
        for name in ("right", "left", "core0"):
            gathers[g][name].start()

    def pass_on(g):
        gathers[g]["right"].wait_recv()
        gathers[g]["right2"].start()
        gathers[g]["left"].wait_recv()
        gathers[g]["left2"].start()
        gathers[g]["core3"].start()
        gathers[g]["core1"].start()

    def close_gather(g):
        gathers[g]["right2"].wait_recv()
        gathers[g]["left2"].wait_recv()
        gathers[g]["core2"].start()
        for name in ("core0", "core1", "core3", "core2"):
            gathers[g][name].wait_recv()

    def multiply(g):
        flat = gathered[g].reshape(-1, width)
        gate_part = jnp.dot(flat, gate[...], preferred_element_type=f32)
        up_part = jnp.dot(flat, up[...], preferred_element_type=f32)
        inner = (gate_part * jax.nn.sigmoid(gate_part) * up_part).astype(bf16)
        share = jnp.dot(inner, down[...], preferred_element_type=f32).astype(bf16)
        partial[g] = share.reshape(2 * Y_RING, block, width)
        for k in (2, 1, 3, 0):
            core_copy(g, k).start()

    def both_cores(g, k, cols):
        return partial[g, 2 * k, :, cols].astype(f32) + from_core[g, k, :, cols].astype(f32)

    def send_halves(g):
        core_copy(g, 2).wait_recv()
        half_sum[g, 0] = both_cores(g, 2, low).astype(bf16)
        half_sum[g, 1] = both_cores(g, 2, high).astype(bf16)
        half_copy(g, 0).start()
        half_copy(g, 1).start()
        core_copy(g, 1).wait_recv()
        whole_sum[g, 0, :, high] = both_cores(g, 1, high).astype(bf16)
        side_copy(g, 0, 1).start()
        core_copy(g, 3).wait_recv()
        whole_sum[g, 1, :, low] = both_cores(g, 3, low).astype(bf16)
        side_copy(g, 1, 0).start()

    def send_sides(g):
        half_copy(g, 0).wait_recv()
        whole_sum[g, 0, :, low] = (both_cores(g, 1, low) + from_half[g, 0].astype(f32)).astype(bf16)
        side_copy(g, 0, 0).start()
        half_copy(g, 1).wait_recv()
        whole_sum[g, 1, :, high] = (both_cores(g, 3, high) + from_half[g, 1].astype(f32)).astype(
            bf16
        )
        side_copy(g, 1, 1).start()

    def give_back(g):
        core_copy(g, 0).wait_recv()
        for way in range(2):
            for part in range(2):
                side_copy(g, way, part).wait_recv()
        total = (
            both_cores(g, 0, slice(None))
            + from_side[g, 0].astype(f32)
            + from_side[g, 1].astype(f32)
        )
        to_tiles(total, words, results, g * block)
        for dz, dx in hops[g]:
            p = place(dz, dx)
            if dz or dx:
                return_copy(dz, dx).start()
            else:
                returned[pl.ds(sp * capacity, capacity)] = results[
                    p * capacity : (p + 1) * capacity
                ]

    open_group(0)
    pass_on(0)
    open_group(1)
    close_gather(0)
    for c in loads:
        c.wait()
    multiply(0)
    pass_on(1)
    send_halves(0)
    close_gather(1)
    multiply(1)
    send_sides(0)
    send_halves(1)
    give_back(0)
    send_sides(1)
    give_back(1)
    for dz, dx in others:
        return_copy(-dz % Z_RING, -dx % X_RING).wait_recv()
    from_tiles(returned, 0, experts * capacity, words, returned_rows)
    column = lax.broadcasted_iota(jnp.int32, (local_rows, experts * capacity), 1)
    routed = jnp.zeros((local_rows, width), f32)
    for c in range(top_count):
        pick = (column == slots_down[:, c : c + 1]).astype(f32).astype(bf16)
        picked = jnp.dot(pick, returned_rows[...], preferred_element_type=f32)
        routed = routed + expert_weight[:, c : c + 1] * picked
    out[...] = layer_norm(
        residual_scale * hidden[...].astype(f32) + routed, norm2_gain[...]
    ).astype(bf16)
    for dz, dx in others:
        dispatch_copy(dz, dx).wait_send()
        return_copy(dz, dx).wait_send()
    for g in range(GROUPS):
        for c in gathers[g].values():
            c.wait_send()
        for k in range(Y_RING):
            core_copy(g, k).wait_send()
        for way in range(2):
            half_copy(g, way).wait_send()
            for part in range(2):
                side_copy(g, way, part).wait_send()


def run_experts(hidden, slots, capacity, expert_weight, norm2_gain, gate_proj, up_proj, down_proj):
    local_rows, width = hidden.shape
    experts = Z_RING * X_RING
    inner = gate_proj.shape[2]
    count = experts * capacity
    block = count // GROUPS
    tall = width // LANES
    vmem = pl.BlockSpec(memory_space=pltpu.VMEM)
    hbm = pl.BlockSpec(memory_space=pl.ANY)
    dma = pltpu.SemaphoreType.DMA
    bf16, f32 = jnp.bfloat16, jnp.float32
    return pl.pallas_call(
        functools.partial(experts_kernel, capacity),
        out_shape=jax.ShapeDtypeStruct((local_rows, width), bf16),
        in_specs=[vmem] * 5 + [hbm] * 3,
        out_specs=vmem,
        scratch_shapes=[
            pltpu.VMEM((width, inner), bf16),
            pltpu.VMEM((width, inner), bf16),
            pltpu.VMEM((inner, width), bf16),
            pltpu.VMEM((count * tall, LANES), f32),
            pltpu.VMEM((count, tall, LANES), bf16),
            pltpu.VMEM((count, tall, LANES), bf16),
            pltpu.VMEM((GROUPS, 2 * Y_RING, block, width), bf16),
            pltpu.VMEM((GROUPS, 2 * Y_RING, block, width), bf16),
            pltpu.VMEM((GROUPS, Y_RING, block, width), bf16),
            pltpu.VMEM((GROUPS, 2, block, width // 2), bf16),
            pltpu.VMEM((GROUPS, 2, block, width // 2), bf16),
            pltpu.VMEM((GROUPS, 2, block, width), bf16),
            pltpu.VMEM((GROUPS, 2, block, width), bf16),
            pltpu.VMEM((count, tall, LANES), bf16),
            pltpu.VMEM((count, tall, LANES), bf16),
            pltpu.VMEM((count, width), bf16),
            dma((3,)),
            dma((experts,)),
            dma((experts,)),
            dma((GROUPS, 8)),
            dma((GROUPS, 8)),
            dma((GROUPS, Y_RING)),
            dma((GROUPS, Y_RING)),
            dma((GROUPS, 2)),
            dma((GROUPS, 2)),
            dma((GROUPS, 2, 2)),
            dma((GROUPS, 2, 2)),
            dma((experts,)),
            dma((experts,)),
        ],
        compiler_params=pltpu.CompilerParams(
            collective_id=1, has_side_effects=True, vmem_limit_bytes=56 * 1024 * 1024
        ),
        name="experts",
    )(
        hidden, jnp.transpose(slots), slots, expert_weight, norm2_gain.reshape(1, -1), gate_proj,
        up_proj, down_proj,
    )


def on_device(
    residual,
    query_narrow,
    key_narrow,
    value_narrow,
    query_wide,
    key_wide,
    value_wide,
    subtract_narrow,
    subtract_wide,
    head_gain,
    out_narrow,
    out_wide,
    norm1_gain,
    norm2_gain,
    expert_ids,
    expert_weight,
    gate_proj,
    up_proj,
    down_proj,
):
    attended = attend(
        query_narrow, key_narrow, value_narrow, query_wide, key_wide, value_wide,
        subtract_narrow, subtract_wide, head_gain,
    )
    mix = mixed_heads(attended, out_narrow, out_wide)
    hidden = layer_norm(residual_scale * residual.astype(jnp.float32) + mix, norm1_gain).astype(
        jnp.bfloat16
    )
    local_rows, top_count = expert_ids.shape
    experts = lax.axis_size("sp")
    capacity = max(2, 3 * local_rows * top_count // (2 * experts))
    flat_ids = expert_ids.reshape(-1)
    onehot = (flat_ids[:, None] == jnp.arange(experts, dtype=jnp.int32)[None, :]).astype(jnp.int32)
    before = jnp.cumsum(onehot, 0) - onehot
    position = jnp.sum(before * onehot, 1)
    slots = (flat_ids * capacity + position).reshape(local_rows, top_count)
    return run_experts(
        hidden, slots, capacity, expert_weight, norm2_gain, gate_proj, up_proj, down_proj
    )


def solution(mesh):
    placed = (
        P(("sp", "tp"), None),
        P("sp", "tp"),
        P("sp", "tp"),
        P("sp", "tp"),
        P("sp", "tp"),
        P("sp", "tp"),
        P("sp", "tp"),
        P("tp"),
        P("tp"),
        P(),
        P(),
        P(),
        P(),
        P(),
        P(("sp", "tp"), None),
        P(("sp", "tp"), None),
        P("sp", None, "tp"),
        P("sp", None, "tp"),
        P("sp", "tp", None),
    )
    return jax.shard_map(
        on_device, mesh=mesh, in_specs=placed, out_specs=P(("sp", "tp"), None), check_vma=False
    )
```

```python
import functools

import jax
import jax.numpy as jnp
from jax import lax
from jax.experimental import pallas as pl
from jax.experimental.pallas import tpu as pltpu
from jax.sharding import PartitionSpec as P

residual_scale = 2.0**0.5
MESH = pl.DeviceIdType.MESH


def layer_norm(values, gain):
    center = jnp.mean(values, -1, keepdims=True)
    spread = jnp.mean(jnp.square(values - center), -1, keepdims=True)
    return (values - center) * lax.rsqrt(spread + 1e-05) * gain


LOG2E = 1.4426950408889634
Z_RING = 8
X_RING = 4
NARROW = (128, 384)
WIDE = (384, 768)
ROW = 896
PLACE = (0, 1, 3, 5, 7, 6, 4, 2)
QPLACE = (3, 1, 0, 2)


Y_RING = 4
STEPS_Z = (0, 1, 7, 4, 2, 6, 3, 5)
GROUPS = 2
LANES = 128


def to_tiles(values, words, target, first):
    rows, width = values.shape
    tall = width // LANES
    for j in range(tall):
        words[pl.ds(j, rows, stride=tall), :] = values[:, LANES * j : LANES * (j + 1)]
    flat = words[0 : rows * tall, :]
    target[first : first + rows] = flat.reshape(rows, tall, LANES).astype(jnp.bfloat16)


def from_tiles(source, first, rows, words, target):
    tall = source.shape[1]
    flat = source[first : first + rows].astype(jnp.float32)
    words[0 : rows * tall, :] = flat.reshape(rows * tall, LANES)
    for j in range(tall):
        target[:, LANES * j : LANES * (j + 1)] = words[pl.ds(j, rows, stride=tall), :].astype(
            jnp.bfloat16
        )


def layer_kernel(
    tok,
    capacity,
    residual,
    query_narrow,
    key_narrow,
    value_narrow,
    query_wide,
    key_wide,
    value_wide,
    subtract_narrow,
    subtract_wide,
    head_gain,
    out_narrow,
    out_wide,
    norm1_gain,
    norm2_gain,
    expert_ids,
    expert_weight,
    gate_proj,
    up_proj,
    down_proj,
    out,
    queries,
    keys,
    top,
    acc,
    stats,
    share,
    share_stats,
    got,
    got_stats,
    attended,
    gathered_heads,
    mix_narrow,
    mix_wide,
    hidden,
    picks,
    gate,
    up,
    down,
    words,
    outgoing,
    received,
    gathered,
    partial,
    from_core,
    half_sum,
    from_half,
    whole_sum,
    from_side,
    results,
    returned,
    returned_rows,
    local_sem,
    q_send,
    q_recv,
    kv_send,
    kv_recv,
    o_send,
    o_recv,
    s_send,
    s_recv,
    a_send,
    a_recv,
    w_sem,
    d_send,
    d_recv,
    g_send,
    g_recv,
    c_send,
    c_recv,
    h_send,
    h_recv,
    f_send,
    f_recv,
    r_send,
    r_recv,
):
    sp = lax.axis_index("sp")
    tp = lax.axis_index("tp")
    heads = lax.axis_size("tp")
    z, x = sp // X_RING, sp % X_RING

    def along_z(k):
        return (lax.rem(z + k, Z_RING) * X_RING + x, tp)

    def along_x(k):
        return (z * X_RING + lax.rem(x + k, X_RING), tp)

    def along_tp(k):
        return (sp, lax.rem(tp + k, heads))

    def expert_at(dz, dx):
        return lax.rem(z + dz, Z_RING) * X_RING + lax.rem(x + dx, X_RING)

    own_q = QPLACE[0] * tok
    loads = [
        pltpu.make_async_copy(src, dst, local_sem.at[i])
        for i, (src, dst) in enumerate(
            (
                (query_narrow, queries.at[pl.ds(own_q, tok), pl.ds(0, 128)]),
                (query_wide, queries.at[pl.ds(own_q, tok), pl.ds(128, 256)]),
                (value_narrow, keys.at[pl.ds(0, tok), pl.ds(128, 128)]),
                (key_narrow, keys.at[pl.ds(0, tok), pl.ds(256, 128)]),
                (key_wide, keys.at[pl.ds(0, tok), pl.ds(384, 256)]),
                (value_wide, keys.at[pl.ds(0, tok), pl.ds(640, 128)]),
            )
        )
    ]
    for c in loads:
        c.start()

    weights = [
        pltpu.make_async_copy(src, dst, w_sem.at[i])
        for i, (src, dst) in enumerate(
            (
                (out_narrow, mix_narrow),
                (out_wide, mix_wide),
                (gate_proj.at[0], gate),
                (up_proj.at[0], up),
                (down_proj.at[0], down),
            )
        )
    ]
    others = [(dz, dx) for dz in STEPS_Z for dx in range(X_RING) if dz or dx]
    barrier = pltpu.get_barrier_semaphore()
    peers = [(expert_at(dz, dx), tp) for dz, dx in others]
    peers = peers + [along_tp(k) for k in range(1, heads)]
    for peer in peers:
        pl.semaphore_signal(barrier, inc=1, device_id=peer, device_id_type=MESH)
    keys[:, 0:128] = jnp.ones((keys.shape[0], 128), jnp.bfloat16)
    keys[:, 768:896] = jnp.ones((keys.shape[0], 128), jnp.bfloat16)
    top[...] = jnp.full(top.shape, -1e30, jnp.float32)
    acc[...] = jnp.zeros(acc.shape, jnp.float32)
    stats[...] = jnp.zeros(stats.shape, jnp.float32)
    for c in loads:
        c.wait()
    pl.semaphore_wait(barrier, len(peers))

    def remote(src, dst, send, recv, peer):
        return pltpu.make_async_remote_copy(
            src_ref=src, dst_ref=dst, send_sem=send, recv_sem=recv, device_id=peer,
            device_id_type=MESH,
        )

    local_rows, top_count = expert_ids.shape
    experts = Z_RING * X_RING

    def choose():
        lane = lax.broadcasted_iota(jnp.int32, (local_rows, experts), 1)
        named = [(expert_ids[:, c : c + 1] == lane).astype(jnp.float32) for c in range(top_count)]
        i = lax.broadcasted_iota(jnp.int32, (local_rows, local_rows), 0)
        j = lax.broadcasted_iota(jnp.int32, (local_rows, local_rows), 1)
        earlier = (j < i).astype(jnp.float32).astype(jnp.bfloat16)
        before = jnp.dot(
            earlier, functools.reduce(jnp.add, named).astype(jnp.bfloat16),
            preferred_element_type=jnp.float32,
        )
        row = lax.broadcasted_iota(jnp.int32, (local_rows, experts * capacity), 1)
        for c in range(top_count):
            position = jnp.sum(before * named[c], -1, keepdims=True)
            slot = expert_ids[:, c : c + 1].astype(jnp.float32) * capacity + position
            picks[c] = (slot == row.astype(jnp.float32)).astype(jnp.float32).astype(jnp.bfloat16)
            before = before + named[c]

    def ring_copy(way, step, piece):
        cols = WIDE if piece else NARROW
        forward = way == 0
        source = (Z_RING - step + 1) % Z_RING if forward else step - 1
        target = (Z_RING - step) % Z_RING if forward else step
        r0, rows = 0, tok
        if 2 * step == Z_RING:
            rows = tok // 2
            r0 = 0 if forward else rows
        at = lambda k: keys.at[
            pl.ds(PLACE[k] * tok + r0, rows), pl.ds(cols[0], cols[1] - cols[0])
        ]
        n = (way * (Z_RING // 2) + step - 1) * 2 + piece
        return remote(
            at(source), at(target), kv_send.at[n], kv_recv.at[n],
            along_z(1 if forward else Z_RING - 1),
        )

    def query_copy(k):
        return remote(
            queries.at[pl.ds(own_q, tok), :],
            queries.at[pl.ds(QPLACE[(X_RING - k) % X_RING] * tok, tok), :],
            q_send.at[k], q_recv.at[k], along_x(k),
        )

    ring = {
        (w, s, p): ring_copy(w, s, p)
        for w in range(2)
        for s in range(1, Z_RING // 2 + 1)
        for p in range(2)
    }
    query_copies = {k: query_copy(k) for k in range(1, X_RING)}

    def start_step(step, piece):
        for w in range(2):
            ring[w, step, piece].start()

    def arrived(step, piece):
        for w in range(2):
            ring[w, step, piece].wait_recv()

    start_step(1, 0)
    for k in (1, 3, 2):
        query_copies[k].start()
    start_step(1, 1)
    for c in weights:
        c.start()
    choose()

    pair = 2 * tok

    def absorb(head, group, k0, span):
        rows = pl.ds(k0, span)
        qrows = pl.ds(group * pair, pair)
        size = 128 if head else 64
        scale = size**-0.5 * LOG2E
        scores = []
        for m in range(2):
            if head:
                q = queries[qrows, 128 + 128 * m : 256 + 128 * m]
                k = keys[rows, 384 + 128 * m : 512 + 128 * m]
            else:
                q = queries[qrows, 0:128]
                lane = lax.broadcasted_iota(jnp.int32, q.shape, 1)
                q = jnp.where((lane < 64) if m == 0 else (lane >= 64), q, jnp.zeros_like(q))
                k = keys[rows, 256:384]
            scores.append(
                lax.dot_general(
                    q, k, (((1,), (1,)), ((), ())), preferred_element_type=jnp.float32
                )
            )
        v = keys[rows, 640:896] if head else keys[rows, 0:256]
        for m in range(2):
            s = scores[m]
            before = top[2 * head + m, qrows, :]
            now = jnp.maximum(before, jnp.max(s, -1, keepdims=True) * scale)
            expo = jnp.exp2(s * scale - now[:, :1])
            shrink = jnp.exp2(before - now)
            add = jnp.dot(expo.astype(jnp.bfloat16), v, preferred_element_type=jnp.float32)
            a = acc[2 * head + m, qrows, :]
            acc[2 * head + m, qrows, :] = (
                jnp.concatenate([a[:, :128] * shrink, a[:, 128:] * shrink], 1) + add
            )
            top[2 * head + m, qrows, :] = now

    def absorb_both(head, k0, span):
        def one(g, carry):
            absorb(head, g, k0, span)
            return carry

        lax.fori_loop(0, 2, one, 0)

    def share_copy(head, k):
        to = (X_RING - k) % X_RING
        n = head * X_RING + k
        return (
            remote(share.at[n], got.at[head * X_RING + to], o_send.at[n], o_recv.at[n], along_x(k)),
            remote(
                share_stats.at[n], got_stats.at[head * X_RING + to], s_send.at[n], s_recv.at[n],
                along_x(k),
            ),
        )

    def finish(head, k):
        n = head * X_RING + k
        qrows = pl.ds(QPLACE[k] * tok, tok)
        lane = lax.broadcasted_iota(jnp.int32, (tok, 128), 1)
        column = jnp.zeros((tok, 128), jnp.float32)
        parts = []
        for m in range(2):
            a = acc[2 * head + m, qrows, :]
            value, total = (a[:, :128], a[:, 128:]) if head else (a[:, 128:], a[:, :128])
            parts.append(value / total)
            column = jnp.where(lane == m, top[2 * head + m, qrows, :] + jnp.log2(total), column)
        both = jnp.concatenate(parts, 1)
        if k == 0:
            got[n] = both.astype(jnp.bfloat16)
        else:
            share[n] = both.astype(jnp.bfloat16)
        stats[0:tok, :] = column
        flat = jnp.transpose(stats[...])[0:8]
        if k == 0:
            got_stats[n] = flat
        else:
            share_stats[n] = flat
            for c in share_copy(head, k):
                c.start()

    def combine(head):
        base = head * X_RING
        for k in range(1, X_RING):
            for c in share_copy(head, k):
                c.wait_recv()
        lse = [got_stats[base + k] for k in range(X_RING)]
        peak = functools.reduce(jnp.maximum, lse)
        weight = [jnp.exp2(v - peak) for v in lse]
        row = lax.broadcasted_iota(jnp.int32, peak.shape, 0)
        factor = jnp.where(row == 1, -(subtract_wide if head else subtract_narrow)[0], 1.0) / functools.reduce(jnp.add, weight)
        wide = jnp.concatenate(
            [w * factor for w in weight]
            + [jnp.zeros((128 - 8 * X_RING, peak.shape[1]), jnp.float32)],
            0,
        )
        turned = jnp.transpose(wide)[0:tok]
        diff = jnp.zeros((tok, 128), jnp.float32)
        for k in range(X_RING):
            o = got[base + k].astype(jnp.float32)
            for m in range(2):
                diff = diff + turned[:, 8 * k + m : 8 * k + m + 1] * o[:, 128 * m : 128 * m + 128]
        spread = jnp.mean(diff * diff, -1, keepdims=True)
        normed = diff * lax.rsqrt(spread + 1e-06) * head_gain[...]
        attended[:, :, 128 * head : 128 * head + 128] = normed.reshape(
            heads, tok // heads, 128
        ).astype(jnp.bfloat16)

    arrived(1, 0)
    start_step(2, 0)
    query_copies[1].wait_recv()
    absorb(0, 1, 0, 256)
    absorb(1, 1, 0, 256)
    query_copies[3].wait_recv()
    query_copies[2].wait_recv()
    absorb(0, 0, 0, 256)
    absorb(1, 0, 0, 256)
    arrived(1, 1)
    start_step(2, 1)
    absorb_both(0, 256, 512)
    absorb_both(1, 256, 512)
    arrived(2, 0)
    start_step(3, 0)
    absorb_both(0, 768, 768)
    arrived(2, 1)
    start_step(3, 1)
    absorb_both(1, 768, 768)
    arrived(3, 0)
    start_step(4, 0)
    absorb_both(0, 1536, 512)
    arrived(3, 1)
    start_step(4, 1)
    absorb_both(1, 1536, 512)
    for head in range(2):
        arrived(4, head)
        absorb(head, 0, 2048, 512)
        finish(head, 2)
        finish(head, 1)
        absorb(head, 1, 2048, 512)
        finish(head, 3)
        finish(head, 0)
    for head in range(2):
        combine(head)

    def head_copy(k):
        return remote(
            attended.at[lax.rem(tp + k, heads)], gathered_heads.at[tp], a_send.at[k], a_recv.at[k],
            along_tp(k),
        )

    for k in range(1, heads):
        head_copy(k).start()
    gathered_heads[pl.ds(tp, 1)] = attended[pl.ds(tp, 1)]
    for k in range(1, heads):
        head_copy(k).wait_recv()
    weights[0].wait()
    weights[1].wait()
    narrow = jnp.concatenate([gathered_heads[t, :, 0:128] for t in range(8)], 1)
    wide = jnp.concatenate([gathered_heads[t, :, 128:256] for t in range(8)], 1)
    mix = jnp.dot(narrow, mix_narrow[...], preferred_element_type=jnp.float32)
    mix = mix + jnp.dot(wide, mix_wide[...], preferred_element_type=jnp.float32)
    hidden[...] = layer_norm(
        residual_scale * residual[...].astype(jnp.float32) + mix, norm1_gain[...]
    ).astype(jnp.bfloat16)

    y, core = tp // 2, tp % 2
    width = hidden.shape[1]
    half = width // 2
    f32, bf16 = jnp.float32, jnp.bfloat16

    def along_y(k):
        return (sp, lax.rem(y + k, Y_RING) * 2 + core)

    sibling = (sp, y * 2 + 1 - core)
    table = functools.reduce(jnp.add, [picks[c] for c in range(top_count)])
    rows = lax.dot_general(
        table, hidden[...], (((0,), (0,)), ((), ())), preferred_element_type=f32
    )
    to_tiles(rows, words, outgoing, 0)

    def place(dz, dx):
        return STEPS_Z.index(dz % Z_RING) * X_RING + dx % X_RING

    def dispatch_copy(dz, dx):
        e = expert_at(dz, dx)
        p = place(-dz, -dx)
        return remote(
            outgoing.at[pl.ds(e * capacity, capacity)],
            received.at[pl.ds(p * capacity, capacity)],
            d_send.at[p], d_recv.at[p], (e, tp),
        )

    def return_copy(dz, dx):
        p = place(dz, dx)
        return remote(
            results.at[pl.ds(p * capacity, capacity)],
            returned.at[pl.ds(sp * capacity, capacity)],
            r_send.at[p], r_recv.at[p], (expert_at(dz, dx), tp),
        )

    per_group = len(STEPS_Z) // GROUPS
    steps_of = [STEPS_Z[g * per_group : (g + 1) * per_group] for g in range(GROUPS)]
    hops = [[(dz, dx) for dz in steps_of[g] for dx in range(X_RING)] for g in range(GROUPS)]
    block = per_group * X_RING * capacity
    low, high = pl.ds(0, half), pl.ds(half, half)

    for g in range(GROUPS):
        for dz, dx in hops[g]:
            if dz or dx:
                dispatch_copy(dz, dx).start()

    def gather_copies(g):
        at = lambda s, c=None: gathered.at[g, s] if c is None else gathered.at[g, s, :, c]
        right, left = along_y(1), along_y(Y_RING - 1)
        plan = {
            "core0": (at(0), at(1), sibling),
            "right": (at(0), at(6), right),
            "left": (at(0), at(2), left),
            "right2": (at(6, low), at(4, low), right),
            "left2": (at(2, high), at(4, high), left),
            "core1": (at(2), at(3), sibling),
            "core3": (at(6), at(7), sibling),
            "core2": (at(4), at(5), sibling),
        }
        return {
            name: remote(src, dst, g_send.at[g, i], g_recv.at[g, i], peer)
            for i, (name, (src, dst, peer)) in enumerate(plan.items())
        }

    gathers = [gather_copies(g) for g in range(GROUPS)]

    def core_copy(g, k):
        return remote(
            partial.at[g, 2 * k + 1], from_core.at[g, k], c_send.at[g, k], c_recv.at[g, k], sibling
        )

    def half_copy(g, way):
        return remote(
            half_sum.at[g, way], from_half.at[g, way], h_send.at[g, way], h_recv.at[g, way],
            along_y(Y_RING - 1 if way else 1),
        )

    def side_copy(g, way, part):
        cols = high if part else low
        return remote(
            whole_sum.at[g, way, :, cols], from_side.at[g, way, :, cols],
            f_send.at[g, way, part], f_recv.at[g, way, part], along_y(Y_RING - 1 if way else 1),
        )

    def open_group(g):
        for dz, dx in hops[g]:
            p = place(dz, dx)
            if dz or dx:
                dispatch_copy(-dz % Z_RING, -dx % X_RING).wait_recv()
            else:
                received[p * capacity : (p + 1) * capacity] = outgoing[
                    pl.ds(sp * capacity, capacity)
                ]
        from_tiles(received, g * block, block, words, gathered.at[g, 0])
        for name in ("right", "left", "core0"):
            gathers[g][name].start()

    def pass_on(g):
        gathers[g]["right"].wait_recv()
        gathers[g]["right2"].start()
        gathers[g]["left"].wait_recv()
        gathers[g]["left2"].start()
        gathers[g]["core3"].start()
        gathers[g]["core1"].start()

    def close_gather(g):
        gathers[g]["right2"].wait_recv()
        gathers[g]["left2"].wait_recv()
        gathers[g]["core2"].start()
        for name in ("core0", "core1", "core3", "core2"):
            gathers[g][name].wait_recv()

    def multiply(g):
        flat = gathered[g].reshape(-1, width)
        gate_part = jnp.dot(flat, gate[...], preferred_element_type=f32)
        up_part = jnp.dot(flat, up[...], preferred_element_type=f32)
        inner = (gate_part * jax.nn.sigmoid(gate_part) * up_part).astype(bf16)
        share = jnp.dot(inner, down[...], preferred_element_type=f32).astype(bf16)
        partial[g] = share.reshape(2 * Y_RING, block, width)
        for k in (2, 1, 3, 0):
            core_copy(g, k).start()

    def both_cores(g, k, cols):
        return partial[g, 2 * k, :, cols].astype(f32) + from_core[g, k, :, cols].astype(f32)

    def send_halves(g):
        core_copy(g, 2).wait_recv()
        half_sum[g, 0] = both_cores(g, 2, low).astype(bf16)
        half_sum[g, 1] = both_cores(g, 2, high).astype(bf16)
        half_copy(g, 0).start()
        half_copy(g, 1).start()
        core_copy(g, 1).wait_recv()
        whole_sum[g, 0, :, high] = both_cores(g, 1, high).astype(bf16)
        side_copy(g, 0, 1).start()
        core_copy(g, 3).wait_recv()
        whole_sum[g, 1, :, low] = both_cores(g, 3, low).astype(bf16)
        side_copy(g, 1, 0).start()

    def send_sides(g):
        half_copy(g, 0).wait_recv()
        whole_sum[g, 0, :, low] = (both_cores(g, 1, low) + from_half[g, 0].astype(f32)).astype(bf16)
        side_copy(g, 0, 0).start()
        half_copy(g, 1).wait_recv()
        whole_sum[g, 1, :, high] = (both_cores(g, 3, high) + from_half[g, 1].astype(f32)).astype(
            bf16
        )
        side_copy(g, 1, 1).start()

    def give_back(g):
        core_copy(g, 0).wait_recv()
        for way in range(2):
            for part in range(2):
                side_copy(g, way, part).wait_recv()
        total = (
            both_cores(g, 0, slice(None))
            + from_side[g, 0].astype(f32)
            + from_side[g, 1].astype(f32)
        )
        to_tiles(total, words, results, g * block)
        for dz, dx in hops[g]:
            p = place(dz, dx)
            if dz or dx:
                return_copy(dz, dx).start()
            else:
                returned[pl.ds(sp * capacity, capacity)] = results[
                    p * capacity : (p + 1) * capacity
                ]

    open_group(0)
    pass_on(0)
    open_group(1)
    close_gather(0)
    for c in weights[2:]:
        c.wait()
    multiply(0)
    pass_on(1)
    send_halves(0)
    close_gather(1)
    multiply(1)
    send_sides(0)
    send_halves(1)
    give_back(0)
    send_sides(1)
    give_back(1)
    for dz, dx in others:
        return_copy(-dz % Z_RING, -dx % X_RING).wait_recv()
    from_tiles(returned, 0, experts * capacity, words, returned_rows)
    routed = jnp.zeros((local_rows, width), f32)
    for c in range(top_count):
        picked = jnp.dot(picks[c], returned_rows[...], preferred_element_type=f32)
        routed = routed + expert_weight[:, c : c + 1] * picked
    out[...] = layer_norm(
        residual_scale * hidden[...].astype(f32) + routed, norm2_gain[...]
    ).astype(bf16)
    for dz, dx in others:
        dispatch_copy(dz, dx).wait_send()
        return_copy(dz, dx).wait_send()
    for g in range(GROUPS):
        for c in gathers[g].values():
            c.wait_send()
        for k in range(Y_RING):
            core_copy(g, k).wait_send()
        for way in range(2):
            half_copy(g, way).wait_send()
            for part in range(2):
                side_copy(g, way, part).wait_send()
    for c in ring.values():
        c.wait_send()
    for c in query_copies.values():
        c.wait_send()
    for head in range(2):
        for k in range(1, X_RING):
            for c in share_copy(head, k):
                c.wait_send()
    for k in range(1, heads):
        head_copy(k).wait_send()


def on_device(
    residual,
    query_narrow,
    key_narrow,
    value_narrow,
    query_wide,
    key_wide,
    value_wide,
    subtract_narrow,
    subtract_wide,
    head_gain,
    out_narrow,
    out_wide,
    norm1_gain,
    norm2_gain,
    expert_ids,
    expert_weight,
    gate_proj,
    up_proj,
    down_proj,
):
    tok = query_narrow.shape[0]
    heads = lax.axis_size("tp")
    lanes = (tok + 127) // 128 * 128
    local_rows, width = residual.shape
    experts = Z_RING * X_RING
    capacity = max(2, 3 * local_rows * expert_ids.shape[1] // (2 * experts))
    inner = gate_proj.shape[2]
    count = experts * capacity
    block = count // GROUPS
    tall = width // LANES
    vmem = pl.BlockSpec(memory_space=pltpu.VMEM)
    smem = pl.BlockSpec(memory_space=pltpu.SMEM)
    hbm = pl.BlockSpec(memory_space=pl.ANY)
    dma = pltpu.SemaphoreType.DMA
    bf16, f32 = jnp.bfloat16, jnp.float32
    return pl.pallas_call(
        functools.partial(layer_kernel, tok, capacity),
        out_shape=jax.ShapeDtypeStruct((local_rows, width), bf16),
        in_specs=[vmem] + [hbm] * 6 + [smem] * 2 + [vmem] + [hbm] * 2 + [vmem] * 4 + [hbm] * 3,
        out_specs=vmem,
        scratch_shapes=[
            pltpu.VMEM((X_RING * tok, 384), bf16),
            pltpu.VMEM((Z_RING * tok, ROW), bf16),
            pltpu.VMEM((4, X_RING * tok, 128), f32),
            pltpu.VMEM((4, X_RING * tok, 256), f32),
            pltpu.VMEM((lanes, 128), f32),
            pltpu.VMEM((2 * X_RING, tok, 256), bf16),
            pltpu.VMEM((2 * X_RING, 8, lanes), f32),
            pltpu.VMEM((2 * X_RING, tok, 256), bf16),
            pltpu.VMEM((2 * X_RING, 8, lanes), f32),
            pltpu.VMEM((heads, tok // heads, 256), bf16),
            pltpu.VMEM((heads, tok // heads, 256), bf16),
            pltpu.VMEM(out_narrow.shape, bf16),
            pltpu.VMEM(out_wide.shape, bf16),
            pltpu.VMEM(residual.shape, bf16),
            pltpu.VMEM((expert_ids.shape[1], local_rows, count), bf16),
            pltpu.VMEM((width, inner), bf16),
            pltpu.VMEM((width, inner), bf16),
            pltpu.VMEM((inner, width), bf16),
            pltpu.VMEM((count * tall, LANES), f32),
            pltpu.VMEM((count, tall, LANES), bf16),
            pltpu.VMEM((count, tall, LANES), bf16),
            pltpu.VMEM((GROUPS, 2 * Y_RING, block, width), bf16),
            pltpu.VMEM((GROUPS, 2 * Y_RING, block, width), bf16),
            pltpu.VMEM((GROUPS, Y_RING, block, width), bf16),
            pltpu.VMEM((GROUPS, 2, block, width // 2), bf16),
            pltpu.VMEM((GROUPS, 2, block, width // 2), bf16),
            pltpu.VMEM((GROUPS, 2, block, width), bf16),
            pltpu.VMEM((GROUPS, 2, block, width), bf16),
            pltpu.VMEM((count, tall, LANES), bf16),
            pltpu.VMEM((count, tall, LANES), bf16),
            pltpu.VMEM((count, width), bf16),
            dma((6,)),
            dma((X_RING,)),
            dma((X_RING,)),
            dma((2 * Z_RING,)),
            dma((2 * Z_RING,)),
            dma((2 * X_RING,)),
            dma((2 * X_RING,)),
            dma((2 * X_RING,)),
            dma((2 * X_RING,)),
            dma((heads,)),
            dma((heads,)),
            dma((5,)),
            dma((experts,)),
            dma((experts,)),
            dma((GROUPS, 8)),
            dma((GROUPS, 8)),
            dma((GROUPS, Y_RING)),
            dma((GROUPS, Y_RING)),
            dma((GROUPS, 2)),
            dma((GROUPS, 2)),
            dma((GROUPS, 2, 2)),
            dma((GROUPS, 2, 2)),
            dma((experts,)),
            dma((experts,)),
        ],
        compiler_params=pltpu.CompilerParams(
            collective_id=0, has_side_effects=True, vmem_limit_bytes=66 * 1000 * 1000
        ),
        name="layer",
    )(
        residual, query_narrow, key_narrow, value_narrow, query_wide, key_wide, value_wide,
        subtract_narrow, subtract_wide, head_gain.reshape(1, -1), out_narrow, out_wide,
        norm1_gain.reshape(1, -1), norm2_gain.reshape(1, -1), expert_ids, expert_weight,
        gate_proj, up_proj, down_proj,
    )


def solution(mesh):
    placed = (
        P(("sp", "tp"), None),
        P("sp", "tp"),
        P("sp", "tp"),
        P("sp", "tp"),
        P("sp", "tp"),
        P("sp", "tp"),
        P("sp", "tp"),
        P("tp"),
        P("tp"),
        P(),
        P(),
        P(),
        P(),
        P(),
        P(("sp", "tp"), None),
        P(("sp", "tp"), None),
        P("sp", None, "tp"),
        P("sp", None, "tp"),
        P("sp", "tp", None),
    )
    return jax.shard_map(
        on_device, mesh=mesh, in_specs=placed, out_specs=P(("sp", "tp"), None), check_vma=False
    )
```

```python
import functools

import jax
import jax.numpy as jnp
from jax import lax
from jax.experimental import pallas as pl
from jax.experimental.pallas import tpu as pltpu
from jax.sharding import PartitionSpec as P

residual_scale = 2.0**0.5
MESH = pl.DeviceIdType.MESH


def layer_norm(values, gain):
    center = jnp.mean(values, -1, keepdims=True)
    spread = jnp.mean(jnp.square(values - center), -1, keepdims=True)
    return (values - center) * lax.rsqrt(spread + 1e-05) * gain


LOG2E = 1.4426950408889634
Z_RING = 8
X_RING = 4
NARROW = (128, 384)
WIDE = (384, 768)
ROW = 896
PLACE = (0, 1, 3, 5, 7, 6, 4, 2)
QPLACE = (3, 1, 0, 2)


Y_RING = 4
LANES = 128


def to_tiles(values, words, target, first):
    rows, width = values.shape
    tall = width // LANES
    for j in range(tall):
        words[pl.ds(j, rows, stride=tall), :] = values[:, LANES * j : LANES * (j + 1)]
    flat = words[0 : rows * tall, :]
    target[first : first + rows] = flat.reshape(rows, tall, LANES).astype(jnp.bfloat16)


def from_tiles(source, first, rows, words, target):
    tall = source.shape[1]
    flat = source[first : first + rows].astype(jnp.float32)
    words[0 : rows * tall, :] = flat.reshape(rows * tall, LANES)
    for j in range(tall):
        target[:, LANES * j : LANES * (j + 1)] = words[pl.ds(j, rows, stride=tall), :].astype(
            jnp.bfloat16
        )


def layer_kernel(
    tok,
    capacity,
    residual,
    query_narrow,
    key_narrow,
    value_narrow,
    query_wide,
    key_wide,
    value_wide,
    subtract_narrow,
    subtract_wide,
    head_gain,
    out_narrow,
    out_wide,
    norm1_gain,
    norm2_gain,
    expert_ids,
    expert_weight,
    gate_proj,
    up_proj,
    down_proj,
    out,
    queries,
    keys,
    top,
    acc,
    stats,
    share,
    share_stats,
    got,
    got_stats,
    attended,
    gathered_heads,
    mix_narrow,
    mix_wide,
    hidden,
    picks,
    scales,
    gate,
    up,
    down,
    words,
    outgoing,
    received,
    gathered,
    partial,
    from_core,
    half_sum,
    from_half,
    whole_sum,
    from_side,
    results,
    returned,
    returned_rows,
    local_sem,
    q_send,
    q_recv,
    kv_send,
    kv_recv,
    o_send,
    o_recv,
    s_send,
    s_recv,
    a_send,
    a_recv,
    w_sem,
    d_send,
    d_recv,
    g_send,
    g_recv,
    c_send,
    c_recv,
    h_send,
    h_recv,
    f_send,
    f_recv,
    r_send,
    r_recv,
):
    sp = lax.axis_index("sp")
    tp = lax.axis_index("tp")
    heads = lax.axis_size("tp")
    z, x = sp // X_RING, sp % X_RING

    def along_z(k):
        return (lax.rem(z + k, Z_RING) * X_RING + x, tp)

    def along_x(k):
        return (z * X_RING + lax.rem(x + k, X_RING), tp)

    def along_tp(k):
        return (sp, lax.rem(tp + k, heads))

    def expert_at(dz, dx):
        return lax.rem(z + dz, Z_RING) * X_RING + lax.rem(x + dx, X_RING)

    own_q = QPLACE[0] * tok
    loads = [
        pltpu.make_async_copy(src, dst, local_sem.at[i])
        for i, (src, dst) in enumerate(
            (
                (query_narrow, queries.at[pl.ds(own_q, tok), pl.ds(0, 128)]),
                (query_wide, queries.at[pl.ds(own_q, tok), pl.ds(128, 256)]),
                (value_narrow, keys.at[pl.ds(0, tok), pl.ds(128, 128)]),
                (key_narrow, keys.at[pl.ds(0, tok), pl.ds(256, 128)]),
                (key_wide, keys.at[pl.ds(0, tok), pl.ds(384, 256)]),
                (value_wide, keys.at[pl.ds(0, tok), pl.ds(640, 128)]),
            )
        )
    ]
    for c in loads:
        c.start()

    weights = [
        pltpu.make_async_copy(src, dst, w_sem.at[i])
        for i, (src, dst) in enumerate(
            (
                (out_narrow, mix_narrow),
                (out_wide, mix_wide),
                (gate_proj.at[0], gate),
                (up_proj.at[0], up),
                (down_proj.at[0], down),
            )
        )
    ]
    others = [(dz, dx) for dz in (4, 3, 5, 2, 6, 1, 7, 0) for dx in range(X_RING) if dz or dx]
    barrier = pltpu.get_barrier_semaphore()
    peers = [along_z(1), along_z(Z_RING - 1)] + [along_x(k) for k in range(1, X_RING)]
    peers = peers + [along_tp(k) for k in range(1, heads)]
    for peer in peers:
        pl.semaphore_signal(barrier, inc=1, device_id=peer, device_id_type=MESH)
    keys[:, 0:128] = jnp.ones((keys.shape[0], 128), jnp.bfloat16)
    keys[:, 768:896] = jnp.ones((keys.shape[0], 128), jnp.bfloat16)
    top[...] = jnp.full(top.shape, -1e30, jnp.float32)
    acc[...] = jnp.zeros(acc.shape, jnp.float32)
    stats[...] = jnp.zeros(stats.shape, jnp.float32)
    for c in loads:
        c.wait()
    pl.semaphore_wait(barrier, len(peers))

    def remote(src, dst, send, recv, peer):
        return pltpu.make_async_remote_copy(
            src_ref=src, dst_ref=dst, send_sem=send, recv_sem=recv, device_id=peer,
            device_id_type=MESH,
        )

    top_count, local_rows = expert_ids.shape
    experts = Z_RING * X_RING

    def choose():
        lane = lax.broadcasted_iota(jnp.int32, (experts, local_rows), 0)
        named = [(expert_ids[c : c + 1, :] == lane).astype(jnp.float32) for c in range(top_count)]
        i = lax.broadcasted_iota(jnp.int32, (local_rows, local_rows), 0)
        j = lax.broadcasted_iota(jnp.int32, (local_rows, local_rows), 1)
        earlier = (i < j).astype(jnp.float32).astype(jnp.bfloat16)
        before = jnp.dot(
            functools.reduce(jnp.add, named).astype(jnp.bfloat16), earlier,
            preferred_element_type=jnp.float32,
        )
        row = lax.broadcasted_iota(jnp.int32, (experts * capacity, local_rows), 0)
        for c in range(top_count):
            position = jnp.sum(before * named[c], 0, keepdims=True)
            slot = position * experts + expert_ids[c : c + 1, :].astype(jnp.float32)
            picks[c] = (slot == row.astype(jnp.float32)).astype(jnp.float32).astype(jnp.bfloat16)
            before = before + named[c]
            own = jnp.where(i == j, expert_weight[c : c + 1, :], 0.0)
            scales[c] = jnp.broadcast_to(jnp.sum(own, 1, keepdims=True), scales.shape[1:])

    def ring_copy(way, step, piece):
        cols = WIDE if piece else NARROW
        forward = way == 0
        source = (Z_RING - step + 1) % Z_RING if forward else step - 1
        target = (Z_RING - step) % Z_RING if forward else step
        r0, rows = 0, tok
        if 2 * step == Z_RING:
            rows = tok // 2
            r0 = 0 if forward else rows
        at = lambda k: keys.at[
            pl.ds(PLACE[k] * tok + r0, rows), pl.ds(cols[0], cols[1] - cols[0])
        ]
        n = (way * (Z_RING // 2) + step - 1) * 2 + piece
        return remote(
            at(source), at(target), kv_send.at[n], kv_recv.at[n],
            along_z(1 if forward else Z_RING - 1),
        )

    def query_copy(k):
        return remote(
            queries.at[pl.ds(own_q, tok), :],
            queries.at[pl.ds(QPLACE[(X_RING - k) % X_RING] * tok, tok), :],
            q_send.at[k], q_recv.at[k], along_x(k),
        )

    ring = {
        (w, s, p): ring_copy(w, s, p)
        for w in range(2)
        for s in range(1, Z_RING // 2 + 1)
        for p in range(2)
    }
    query_copies = {k: query_copy(k) for k in range(1, X_RING)}

    def start_step(step, piece):
        for w in range(2):
            ring[w, step, piece].start()

    def arrived(step, piece):
        for w in range(2):
            ring[w, step, piece].wait_recv()

    start_step(1, 0)
    for k in (1, 3, 2):
        query_copies[k].start()
    start_step(1, 1)
    for c in weights:
        c.start()
    choose()

    pair = 2 * tok

    def absorb(head, group, k0, span):
        rows = pl.ds(k0, span)
        qrows = pl.ds(group * pair, pair)
        size = 128 if head else 64
        scale = size**-0.5 * LOG2E
        scores = []
        for m in range(2):
            if head:
                q = queries[qrows, 128 + 128 * m : 256 + 128 * m]
                k = keys[rows, 384 + 128 * m : 512 + 128 * m]
            else:
                q = queries[qrows, 0:128]
                lane = lax.broadcasted_iota(jnp.int32, q.shape, 1)
                q = jnp.where((lane < 64) if m == 0 else (lane >= 64), q, jnp.zeros_like(q))
                k = keys[rows, 256:384]
            scores.append(
                lax.dot_general(
                    q, k, (((1,), (1,)), ((), ())), preferred_element_type=jnp.float32
                )
            )
        v = keys[rows, 640:896] if head else keys[rows, 0:256]
        for m in range(2):
            s = scores[m]
            before = top[2 * head + m, qrows, :]
            now = jnp.maximum(before, jnp.max(s, -1, keepdims=True) * scale)
            expo = jnp.exp2(s * scale - now[:, :1])
            shrink = jnp.exp2(before - now)
            add = jnp.dot(expo.astype(jnp.bfloat16), v, preferred_element_type=jnp.float32)
            a = acc[2 * head + m, qrows, :]
            acc[2 * head + m, qrows, :] = (
                jnp.concatenate([a[:, :128] * shrink, a[:, 128:] * shrink], 1) + add
            )
            top[2 * head + m, qrows, :] = now

    def absorb_both(head, k0, span):
        def one(g, carry):
            absorb(head, g, k0, span)
            return carry

        lax.fori_loop(0, 2, one, 0)

    def share_copy(head, k):
        to = (X_RING - k) % X_RING
        n = head * X_RING + k
        return (
            remote(share.at[n], got.at[head * X_RING + to], o_send.at[n], o_recv.at[n], along_x(k)),
            remote(
                share_stats.at[n], got_stats.at[head * X_RING + to], s_send.at[n], s_recv.at[n],
                along_x(k),
            ),
        )

    def finish(head, k):
        n = head * X_RING + k
        qrows = pl.ds(QPLACE[k] * tok, tok)
        lane = lax.broadcasted_iota(jnp.int32, (tok, 128), 1)
        column = jnp.zeros((tok, 128), jnp.float32)
        parts = []
        for m in range(2):
            a = acc[2 * head + m, qrows, :]
            value, total = (a[:, :128], a[:, 128:]) if head else (a[:, 128:], a[:, :128])
            parts.append(value / total)
            column = jnp.where(lane == m, top[2 * head + m, qrows, :] + jnp.log2(total), column)
        both = jnp.concatenate(parts, 1)
        if k == 0:
            got[n] = both.astype(jnp.bfloat16)
        else:
            share[n] = both.astype(jnp.bfloat16)
        stats[0:tok, :] = column
        flat = jnp.transpose(stats[...])[0:8]
        if k == 0:
            got_stats[n] = flat
        else:
            share_stats[n] = flat
            for c in share_copy(head, k):
                c.start()

    def combine(head):
        base = head * X_RING
        for k in range(1, X_RING):
            for c in share_copy(head, k):
                c.wait_recv()
        lse = [got_stats[base + k] for k in range(X_RING)]
        peak = functools.reduce(jnp.maximum, lse)
        weight = [jnp.exp2(v - peak) for v in lse]
        row = lax.broadcasted_iota(jnp.int32, peak.shape, 0)
        factor = jnp.where(row == 1, -(subtract_wide if head else subtract_narrow)[0], 1.0) / functools.reduce(jnp.add, weight)
        wide = jnp.concatenate(
            [w * factor for w in weight]
            + [jnp.zeros((128 - 8 * X_RING, peak.shape[1]), jnp.float32)],
            0,
        )
        turned = jnp.transpose(wide)[0:tok]
        diff = jnp.zeros((tok, 128), jnp.float32)
        for k in range(X_RING):
            o = got[base + k].astype(jnp.float32)
            for m in range(2):
                diff = diff + turned[:, 8 * k + m : 8 * k + m + 1] * o[:, 128 * m : 128 * m + 128]
        spread = jnp.mean(diff * diff, -1, keepdims=True)
        normed = diff * lax.rsqrt(spread + 1e-06) * head_gain[...]
        attended[:, :, 128 * head : 128 * head + 128] = normed.reshape(
            heads, tok // heads, 128
        ).astype(jnp.bfloat16)

    arrived(1, 0)
    start_step(2, 0)
    query_copies[3].wait_recv()
    query_copies[1].wait_recv()
    for head in range(2):
        absorb(head, 1, 0, 256)
    arrived(1, 1)
    start_step(2, 1)
    for head in range(2):
        absorb(head, 1, 256, 512)
    arrived(2, 0)
    start_step(3, 0)
    query_copies[2].wait_recv()
    for head in range(2):
        absorb(head, 0, 0, 768)
    arrived(2, 1)
    start_step(3, 1)
    absorb_both(0, 768, 768)
    arrived(3, 0)
    start_step(4, 0)
    absorb_both(1, 768, 768)
    absorb(0, 0, 1536, 512)
    arrived(3, 1)
    start_step(4, 1)
    absorb(0, 1, 1536, 512)
    absorb_both(1, 1536, 512)
    for head in range(2):
        arrived(4, head)
        absorb(head, 0, 2048, 512)
        finish(head, 2)
        finish(head, 1)
        absorb(head, 1, 2048, 512)
        finish(head, 3)
        finish(head, 0)
    for head in range(2):
        combine(head)

    def head_copy(k):
        return remote(
            attended.at[lax.rem(tp + k, heads)], gathered_heads.at[tp], a_send.at[k], a_recv.at[k],
            along_tp(k),
        )

    for k in range(1, heads):
        head_copy(k).start()
    gathered_heads[pl.ds(tp, 1)] = attended[pl.ds(tp, 1)]
    for k in range(1, heads):
        head_copy(k).wait_recv()
    weights[0].wait()
    weights[1].wait()
    narrow = jnp.concatenate([gathered_heads[t, :, 0:128] for t in range(8)], 1)
    wide = jnp.concatenate([gathered_heads[t, :, 128:256] for t in range(8)], 1)
    mix = jnp.dot(narrow, mix_narrow[...], preferred_element_type=jnp.float32)
    mix = mix + jnp.dot(wide, mix_wide[...], preferred_element_type=jnp.float32)
    hidden[...] = layer_norm(
        residual_scale * residual[...].astype(jnp.float32) + mix, norm1_gain[...]
    ).astype(jnp.bfloat16)

    y, core = tp // 2, tp % 2
    width = hidden.shape[1]
    half = width // 2
    f32, bf16 = jnp.float32, jnp.bfloat16

    def along_y(k):
        return (sp, lax.rem(y + k, Y_RING) * 2 + core)

    sibling = (sp, y * 2 + 1 - core)
    table = functools.reduce(jnp.add, [picks[c] for c in range(top_count)])
    rows = jnp.dot(table, hidden[...], preferred_element_type=f32)
    to_tiles(rows, words, outgoing, 0)

    def place(dz, dx):
        return dz % Z_RING * X_RING + dx % X_RING

    def dispatch_copy(g, dz, dx):
        e = expert_at(dz, dx)
        p = place(-dz, -dx)
        return remote(
            outgoing.at[g * experts + e], received.at[g * experts + p],
            d_send.at[g, p], d_recv.at[g, p], (e, tp),
        )

    def return_copy(g, dz, dx):
        p = place(dz, dx)
        return remote(
            results.at[g * experts + p], returned.at[g * experts + sp],
            r_send.at[g, p], r_recv.at[g, p], (expert_at(dz, dx), tp),
        )

    block = experts
    low, high = pl.ds(0, half), pl.ds(half, half)

    for g in range(capacity):
        for dz, dx in others:
            dispatch_copy(g, dz, dx).start()

    def gather_copies(g):
        at = lambda s, c=None: gathered.at[g, s] if c is None else gathered.at[g, s, :, c]
        right, left = along_y(1), along_y(Y_RING - 1)
        plan = {
            "core0": (at(0), at(1), sibling),
            "right": (at(0), at(6), right),
            "left": (at(0), at(2), left),
            "right2": (at(6, low), at(4, low), right),
            "left2": (at(2, high), at(4, high), left),
            "core1": (at(2), at(3), sibling),
            "core3": (at(6), at(7), sibling),
            "core2": (at(4), at(5), sibling),
        }
        return {
            name: remote(src, dst, g_send.at[g, i], g_recv.at[g, i], peer)
            for i, (name, (src, dst, peer)) in enumerate(plan.items())
        }

    gathers = [gather_copies(g) for g in range(capacity)]

    def core_copy(g, k):
        return remote(
            partial.at[g, 2 * k + 1], from_core.at[g, k], c_send.at[g, k], c_recv.at[g, k], sibling
        )

    def half_copy(g, way):
        return remote(
            half_sum.at[g, way], from_half.at[g, way], h_send.at[g, way], h_recv.at[g, way],
            along_y(Y_RING - 1 if way else 1),
        )

    def side_copy(g, way, part):
        cols = high if part else low
        return remote(
            whole_sum.at[g, way, :, cols], from_side.at[g, way, :, cols],
            f_send.at[g, way, part], f_recv.at[g, way, part], along_y(Y_RING - 1 if way else 1),
        )

    def open_group(g):
        received[g * experts] = outgoing[g * experts + sp]
        for dz, dx in others:
            dispatch_copy(g, -dz % Z_RING, -dx % X_RING).wait_recv()
        from_tiles(received, g * block, block, words, gathered.at[g, 0])
        for name in ("right", "left", "core0"):
            gathers[g][name].start()

    def pass_on(g):
        gathers[g]["right"].wait_recv()
        gathers[g]["right2"].start()
        gathers[g]["left"].wait_recv()
        gathers[g]["left2"].start()
        gathers[g]["core3"].start()
        gathers[g]["core1"].start()

    def close_gather(g):
        gathers[g]["right2"].wait_recv()
        gathers[g]["left2"].wait_recv()
        gathers[g]["core2"].start()
        for name in ("core0", "core1", "core3", "core2"):
            gathers[g][name].wait_recv()

    def multiply(g):
        flat = gathered[g].reshape(-1, width)
        gate_part = jnp.dot(flat, gate[...], preferred_element_type=f32)
        up_part = jnp.dot(flat, up[...], preferred_element_type=f32)
        inner = (gate_part * jax.nn.sigmoid(gate_part) * up_part).astype(bf16)
        share = jnp.dot(inner, down[...], preferred_element_type=f32).astype(bf16)
        partial[g] = share.reshape(2 * Y_RING, block, width)
        for k in (2, 1, 3, 0):
            core_copy(g, k).start()

    def both_cores(g, k, cols):
        return partial[g, 2 * k, :, cols].astype(f32) + from_core[g, k, :, cols].astype(f32)

    def send_halves(g):
        core_copy(g, 2).wait_recv()
        half_sum[g, 0] = both_cores(g, 2, low).astype(bf16)
        half_sum[g, 1] = both_cores(g, 2, high).astype(bf16)
        half_copy(g, 0).start()
        half_copy(g, 1).start()
        core_copy(g, 1).wait_recv()
        whole_sum[g, 0, :, high] = both_cores(g, 1, high).astype(bf16)
        side_copy(g, 0, 1).start()
        core_copy(g, 3).wait_recv()
        whole_sum[g, 1, :, low] = both_cores(g, 3, low).astype(bf16)
        side_copy(g, 1, 0).start()

    def send_sides(g):
        half_copy(g, 0).wait_recv()
        whole_sum[g, 0, :, low] = (both_cores(g, 1, low) + from_half[g, 0].astype(f32)).astype(bf16)
        side_copy(g, 0, 0).start()
        half_copy(g, 1).wait_recv()
        whole_sum[g, 1, :, high] = (both_cores(g, 3, high) + from_half[g, 1].astype(f32)).astype(
            bf16
        )
        side_copy(g, 1, 1).start()

    def give_back(g):
        core_copy(g, 0).wait_recv()
        for way in range(2):
            for part in range(2):
                side_copy(g, way, part).wait_recv()
        total = (
            both_cores(g, 0, slice(None))
            + from_side[g, 0].astype(f32)
            + from_side[g, 1].astype(f32)
        )
        to_tiles(total, words, results, g * block)
        for dz, dx in others:
            return_copy(g, dz, dx).start()
        returned[g * experts + sp] = results[g * experts]

    open_group(0)
    open_group(1)
    pass_on(0)
    open_group(2)
    pass_on(1)
    for c in weights[2:]:
        c.wait()
    close_gather(0)
    multiply(0)
    pass_on(2)
    send_halves(0)
    close_gather(1)
    multiply(1)
    send_sides(0)
    send_halves(1)
    close_gather(2)
    multiply(2)
    give_back(0)
    send_sides(1)
    send_halves(2)
    give_back(1)
    send_sides(2)
    give_back(2)
    for g in range(capacity):
        for dz, dx in others:
            return_copy(g, -dz % Z_RING, -dx % X_RING).wait_recv()
    from_tiles(returned, 0, experts * capacity, words, returned_rows)
    routed = jnp.zeros((local_rows, width), f32)
    for c in range(top_count):
        picked = lax.dot_general(
            picks[c], returned_rows[...], (((0,), (0,)), ((), ())), preferred_element_type=f32
        )
        routed = routed + scales[c, :, 0:1] * picked
    out[...] = layer_norm(
        residual_scale * hidden[...].astype(f32) + routed, norm2_gain[...]
    ).astype(bf16)
    for g in range(capacity):
        for dz, dx in others:
            dispatch_copy(g, dz, dx).wait_send()
            return_copy(g, dz, dx).wait_send()
        for c in gathers[g].values():
            c.wait_send()
        for k in range(Y_RING):
            core_copy(g, k).wait_send()
        for way in range(2):
            half_copy(g, way).wait_send()
            for part in range(2):
                side_copy(g, way, part).wait_send()
    for c in ring.values():
        c.wait_send()
    for c in query_copies.values():
        c.wait_send()
    for head in range(2):
        for k in range(1, X_RING):
            for c in share_copy(head, k):
                c.wait_send()
    for k in range(1, heads):
        head_copy(k).wait_send()


def on_device(
    residual,
    query_narrow,
    key_narrow,
    value_narrow,
    query_wide,
    key_wide,
    value_wide,
    subtract_narrow,
    subtract_wide,
    head_gain,
    out_narrow,
    out_wide,
    norm1_gain,
    norm2_gain,
    expert_ids,
    expert_weight,
    gate_proj,
    up_proj,
    down_proj,
):
    tok = query_narrow.shape[0]
    heads = lax.axis_size("tp")
    lanes = (tok + 127) // 128 * 128
    local_rows, width = residual.shape
    experts = Z_RING * X_RING
    capacity = max(2, 3 * local_rows * expert_ids.shape[1] // (2 * experts))
    inner = gate_proj.shape[2]
    count = experts * capacity
    block = experts
    tall = width // LANES
    vmem = pl.BlockSpec(memory_space=pltpu.VMEM)
    smem = pl.BlockSpec(memory_space=pltpu.SMEM)
    hbm = pl.BlockSpec(memory_space=pl.ANY)
    dma = pltpu.SemaphoreType.DMA
    bf16, f32 = jnp.bfloat16, jnp.float32
    return pl.pallas_call(
        functools.partial(layer_kernel, tok, capacity),
        out_shape=jax.ShapeDtypeStruct((local_rows, width), bf16),
        in_specs=[vmem] + [hbm] * 6 + [smem] * 2 + [vmem] + [hbm] * 2 + [vmem] * 4 + [hbm] * 3,
        out_specs=vmem,
        scratch_shapes=[
            pltpu.VMEM((X_RING * tok, 384), bf16),
            pltpu.VMEM((Z_RING * tok, ROW), bf16),
            pltpu.VMEM((4, X_RING * tok, 128), f32),
            pltpu.VMEM((4, X_RING * tok, 256), f32),
            pltpu.VMEM((lanes, 128), f32),
            pltpu.VMEM((2 * X_RING, tok, 256), bf16),
            pltpu.VMEM((2 * X_RING, 8, lanes), f32),
            pltpu.VMEM((2 * X_RING, tok, 256), bf16),
            pltpu.VMEM((2 * X_RING, 8, lanes), f32),
            pltpu.VMEM((heads, tok // heads, 256), bf16),
            pltpu.VMEM((heads, tok // heads, 256), bf16),
            pltpu.VMEM(out_narrow.shape, bf16),
            pltpu.VMEM(out_wide.shape, bf16),
            pltpu.VMEM(residual.shape, bf16),
            pltpu.VMEM((expert_ids.shape[1], count, local_rows), bf16),
            pltpu.VMEM((expert_ids.shape[1], local_rows, LANES), f32),
            pltpu.VMEM((width, inner), bf16),
            pltpu.VMEM((width, inner), bf16),
            pltpu.VMEM((inner, width), bf16),
            pltpu.VMEM((count * tall, LANES), f32),
            pltpu.VMEM((count, tall, LANES), bf16),
            pltpu.VMEM((count, tall, LANES), bf16),
            pltpu.VMEM((capacity, 2 * Y_RING, block, width), bf16),
            pltpu.VMEM((capacity, 2 * Y_RING, block, width), bf16),
            pltpu.VMEM((capacity, Y_RING, block, width), bf16),
            pltpu.VMEM((capacity, 2, block, width // 2), bf16),
            pltpu.VMEM((capacity, 2, block, width // 2), bf16),
            pltpu.VMEM((capacity, 2, block, width), bf16),
            pltpu.VMEM((capacity, 2, block, width), bf16),
            pltpu.VMEM((count, tall, LANES), bf16),
            pltpu.VMEM((count, tall, LANES), bf16),
            pltpu.VMEM((count, width), bf16),
            dma((6,)),
            dma((X_RING,)),
            dma((X_RING,)),
            dma((2 * Z_RING,)),
            dma((2 * Z_RING,)),
            dma((2 * X_RING,)),
            dma((2 * X_RING,)),
            dma((2 * X_RING,)),
            dma((2 * X_RING,)),
            dma((heads,)),
            dma((heads,)),
            dma((5,)),
            dma((capacity, experts)),
            dma((capacity, experts)),
            dma((capacity, 8)),
            dma((capacity, 8)),
            dma((capacity, Y_RING)),
            dma((capacity, Y_RING)),
            dma((capacity, 2)),
            dma((capacity, 2)),
            dma((capacity, 2, 2)),
            dma((capacity, 2, 2)),
            dma((capacity, experts)),
            dma((capacity, experts)),
        ],
        compiler_params=pltpu.CompilerParams(
            collective_id=0, has_side_effects=True, vmem_limit_bytes=66 * 1000 * 1000
        ),
        name="layer",
    )(
        residual, query_narrow, key_narrow, value_narrow, query_wide, key_wide, value_wide,
        subtract_narrow, subtract_wide, head_gain.reshape(1, -1), out_narrow, out_wide,
        norm1_gain.reshape(1, -1), norm2_gain.reshape(1, -1), jnp.transpose(expert_ids),
        jnp.transpose(expert_weight), gate_proj, up_proj, down_proj,
    )


def solution(mesh):
    placed = (
        P(("sp", "tp"), None),
        P("sp", "tp"),
        P("sp", "tp"),
        P("sp", "tp"),
        P("sp", "tp"),
        P("sp", "tp"),
        P("sp", "tp"),
        P("tp"),
        P("tp"),
        P(),
        P(),
        P(),
        P(),
        P(),
        P(("sp", "tp"), None),
        P(("sp", "tp"), None),
        P("sp", None, "tp"),
        P("sp", None, "tp"),
        P("sp", "tp", None),
    )
    return jax.shard_map(
        on_device, mesh=mesh, in_specs=placed, out_specs=P(("sp", "tp"), None), check_vma=False
    )
```

```python
import functools

import jax
import jax.numpy as jnp
from jax import lax
from jax.experimental import pallas as pl
from jax.experimental.pallas import tpu as pltpu
from jax.sharding import PartitionSpec as P

residual_scale = 2.0**0.5
MESH = pl.DeviceIdType.MESH


def layer_norm(values, gain):
    center = jnp.mean(values, -1, keepdims=True)
    spread = jnp.mean(jnp.square(values - center), -1, keepdims=True)
    return (values - center) * lax.rsqrt(spread + 1e-05) * gain


LOG2E = 1.4426950408889634
Z_RING = 8
X_RING = 4
NARROW = (128, 384)
WIDE = (384, 768)
ROW = 896
PLACE = (0, 1, 3, 5, 7, 6, 4, 2)
QPLACE = (3, 1, 0, 2)


Y_RING = 4
LANES = 128


def to_tiles(values, words, target, first):
    rows, width = values.shape
    tall = width // LANES
    for j in range(tall):
        words[pl.ds(j, rows, stride=tall), :] = values[:, LANES * j : LANES * (j + 1)]
    flat = words[0 : rows * tall, :]
    target[first : first + rows] = flat.reshape(rows, tall, LANES).astype(jnp.bfloat16)


def from_tiles(source, first, rows, words, target):
    tall = source.shape[1]
    flat = source[first : first + rows].astype(jnp.float32)
    words[0 : rows * tall, :] = flat.reshape(rows * tall, LANES)
    for j in range(tall):
        target[:, LANES * j : LANES * (j + 1)] = words[pl.ds(j, rows, stride=tall), :].astype(
            jnp.bfloat16
        )


def layer_kernel(
    tok,
    capacity,
    residual,
    query_narrow,
    key_narrow,
    value_narrow,
    query_wide,
    key_wide,
    value_wide,
    subtract_narrow,
    subtract_wide,
    head_gain,
    out_narrow,
    out_wide,
    norm1_gain,
    norm2_gain,
    expert_ids,
    expert_weight,
    gate_proj,
    up_proj,
    down_proj,
    out,
    queries,
    keys,
    top,
    acc,
    stats,
    share,
    share_stats,
    got,
    got_stats,
    attended,
    gathered_heads,
    mix_narrow,
    mix_wide,
    hidden,
    picks,
    scales,
    gate,
    up,
    down,
    words,
    outgoing,
    received,
    gathered,
    partial,
    from_core,
    half_sum,
    from_half,
    whole_sum,
    from_side,
    results,
    returned,
    returned_rows,
    local_sem,
    q_send,
    q_recv,
    kv_send,
    kv_recv,
    o_send,
    o_recv,
    s_send,
    s_recv,
    a_send,
    a_recv,
    w_sem,
    d_send,
    d_recv,
    g_send,
    g_recv,
    c_send,
    c_recv,
    h_send,
    h_recv,
    f_send,
    f_recv,
    r_send,
    r_recv,
):
    sp = lax.axis_index("sp")
    tp = lax.axis_index("tp")
    heads = lax.axis_size("tp")
    z, x = sp // X_RING, sp % X_RING

    def along_z(k):
        return (lax.rem(z + k, Z_RING) * X_RING + x, tp)

    def along_x(k):
        return (z * X_RING + lax.rem(x + k, X_RING), tp)

    def along_tp(k):
        return (sp, lax.rem(tp + k, heads))

    def expert_at(dz, dx):
        return lax.rem(z + dz, Z_RING) * X_RING + lax.rem(x + dx, X_RING)

    own_q = QPLACE[0] * tok
    loads = [
        pltpu.make_async_copy(src, dst, local_sem.at[i])
        for i, (src, dst) in enumerate(
            (
                (query_narrow, queries.at[pl.ds(own_q, tok), pl.ds(0, 128)]),
                (query_wide, queries.at[pl.ds(own_q, tok), pl.ds(128, 256)]),
                (value_narrow, keys.at[pl.ds(0, tok), pl.ds(128, 128)]),
                (key_narrow, keys.at[pl.ds(0, tok), pl.ds(256, 128)]),
                (key_wide, keys.at[pl.ds(0, tok), pl.ds(384, 256)]),
                (value_wide, keys.at[pl.ds(0, tok), pl.ds(640, 128)]),
            )
        )
    ]
    for c in loads:
        c.start()

    weights = [
        pltpu.make_async_copy(src, dst, w_sem.at[i])
        for i, (src, dst) in enumerate(
            (
                (out_narrow, mix_narrow),
                (out_wide, mix_wide),
                (gate_proj.at[0], gate),
                (up_proj.at[0], up),
                (down_proj.at[0], down),
            )
        )
    ]
    others = [(dz, dx) for dz in (4, 3, 5, 2, 6, 1, 7, 0) for dx in range(X_RING) if dz or dx]
    barrier = pltpu.get_barrier_semaphore()
    peers = [along_z(1), along_z(Z_RING - 1)] + [along_x(k) for k in range(1, X_RING)]
    peers = peers + [along_tp(k) for k in range(1, heads)]
    for peer in peers:
        pl.semaphore_signal(barrier, inc=1, device_id=peer, device_id_type=MESH)
    keys[:, 0:128] = jnp.ones((keys.shape[0], 128), jnp.bfloat16)
    keys[:, 768:896] = jnp.ones((keys.shape[0], 128), jnp.bfloat16)
    top[...] = jnp.full(top.shape, -1e30, jnp.float32)
    acc[...] = jnp.zeros(acc.shape, jnp.float32)
    stats[...] = jnp.zeros(stats.shape, jnp.float32)
    for c in loads:
        c.wait()
    pl.semaphore_wait(barrier, len(peers))

    def remote(src, dst, send, recv, peer):
        return pltpu.make_async_remote_copy(
            src_ref=src, dst_ref=dst, send_sem=send, recv_sem=recv, device_id=peer,
            device_id_type=MESH,
        )

    top_count, local_rows = expert_ids.shape
    experts = Z_RING * X_RING

    def choose():
        lane = lax.broadcasted_iota(jnp.int32, (experts, local_rows), 0)
        named = [(expert_ids[c : c + 1, :] == lane).astype(jnp.float32) for c in range(top_count)]
        i = lax.broadcasted_iota(jnp.int32, (local_rows, local_rows), 0)
        j = lax.broadcasted_iota(jnp.int32, (local_rows, local_rows), 1)
        earlier = (i < j).astype(jnp.float32).astype(jnp.bfloat16)
        before = jnp.dot(
            functools.reduce(jnp.add, named).astype(jnp.bfloat16), earlier,
            preferred_element_type=jnp.float32,
        )
        row = lax.broadcasted_iota(jnp.int32, (experts * capacity, local_rows), 0)
        for c in range(top_count):
            position = jnp.sum(before * named[c], 0, keepdims=True)
            slot = position * experts + expert_ids[c : c + 1, :].astype(jnp.float32)
            picks[c] = (slot == row.astype(jnp.float32)).astype(jnp.float32).astype(jnp.bfloat16)
            before = before + named[c]
            own = jnp.where(i == j, expert_weight[c : c + 1, :], 0.0)
            scales[c] = jnp.broadcast_to(jnp.sum(own, 1, keepdims=True), scales.shape[1:])

    def ring_copy(way, step, piece):
        cols = WIDE if piece else NARROW
        forward = way == 0
        source = (Z_RING - step + 1) % Z_RING if forward else step - 1
        target = (Z_RING - step) % Z_RING if forward else step
        r0, rows = 0, tok
        if piece or 2 * step == Z_RING:
            rows = tok // 2
            r0 = 0 if forward == (piece < 2) else rows
        at = lambda k: keys.at[
            pl.ds(PLACE[k] * tok + r0, rows), pl.ds(cols[0], cols[1] - cols[0])
        ]
        n = (way * (Z_RING // 2) + step - 1) * 3 + piece
        return remote(
            at(source), at(target), kv_send.at[n], kv_recv.at[n],
            along_z(1 if forward else Z_RING - 1),
        )

    def query_copy(k):
        return remote(
            queries.at[pl.ds(own_q, tok), :],
            queries.at[pl.ds(QPLACE[(X_RING - k) % X_RING] * tok, tok), :],
            q_send.at[k], q_recv.at[k], along_x(k),
        )

    ring = {
        (w, s, p): ring_copy(w, s, p)
        for w in range(2)
        for s in range(1, Z_RING // 2 + 1)
        for p in range(3 if 2 * s < Z_RING else 2)
    }
    query_copies = {k: query_copy(k) for k in range(1, X_RING)}

    def start_step(step, piece):
        for w in range(2):
            ring[w, step, piece].start()

    def arrived(step, piece):
        for w in range(2):
            ring[w, step, piece].wait_recv()

    def pass_on_keys(step, piece):
        for w in range(2):
            ring[w, step, piece].wait_recv()
            ring[w, step + 1, piece].start()

    start_step(1, 0)
    for k in (1, 3, 2):
        query_copies[k].start()
    start_step(1, 1)
    for c in weights:
        c.start()
    choose()

    pair = 2 * tok

    def absorb(head, group, k0, span):
        rows = pl.ds(k0, span)
        qrows = pl.ds(group * pair, pair)
        size = 128 if head else 64
        scale = size**-0.5 * LOG2E
        scores = []
        for m in range(2):
            if head:
                q = queries[qrows, 128 + 128 * m : 256 + 128 * m]
                k = keys[rows, 384 + 128 * m : 512 + 128 * m]
            else:
                q = queries[qrows, 0:128]
                lane = lax.broadcasted_iota(jnp.int32, q.shape, 1)
                q = jnp.where((lane < 64) if m == 0 else (lane >= 64), q, jnp.zeros_like(q))
                k = keys[rows, 256:384]
            scores.append(
                lax.dot_general(
                    q, k, (((1,), (1,)), ((), ())), preferred_element_type=jnp.float32
                )
            )
        v = keys[rows, 640:896] if head else keys[rows, 0:256]
        for m in range(2):
            s = scores[m]
            before = top[2 * head + m, qrows, :]
            now = jnp.maximum(before, jnp.max(s, -1, keepdims=True) * scale)
            expo = jnp.exp2(s * scale - now[:, :1])
            shrink = jnp.exp2(before - now)
            add = jnp.dot(expo.astype(jnp.bfloat16), v, preferred_element_type=jnp.float32)
            a = acc[2 * head + m, qrows, :]
            acc[2 * head + m, qrows, :] = (
                jnp.concatenate([a[:, :128] * shrink, a[:, 128:] * shrink], 1) + add
            )
            top[2 * head + m, qrows, :] = now

    def absorb_both(head, k0, span):
        def one(g, carry):
            absorb(head, g, k0, span)
            return carry

        lax.fori_loop(0, 2, one, 0)

    def share_copy(head, k):
        to = (X_RING - k) % X_RING
        n = head * X_RING + k
        return (
            remote(share.at[n], got.at[head * X_RING + to], o_send.at[n], o_recv.at[n], along_x(k)),
            remote(
                share_stats.at[n], got_stats.at[head * X_RING + to], s_send.at[n], s_recv.at[n],
                along_x(k),
            ),
        )

    def finish(head, k):
        n = head * X_RING + k
        qrows = pl.ds(QPLACE[k] * tok, tok)
        lane = lax.broadcasted_iota(jnp.int32, (tok, 128), 1)
        column = jnp.zeros((tok, 128), jnp.float32)
        parts = []
        for m in range(2):
            a = acc[2 * head + m, qrows, :]
            value, total = (a[:, :128], a[:, 128:]) if head else (a[:, 128:], a[:, :128])
            parts.append(value / total)
            column = jnp.where(lane == m, top[2 * head + m, qrows, :] + jnp.log2(total), column)
        both = jnp.concatenate(parts, 1)
        if k == 0:
            got[n] = both.astype(jnp.bfloat16)
        else:
            share[n] = both.astype(jnp.bfloat16)
        stats[0:tok, :] = column
        flat = jnp.transpose(stats[...])[0:8]
        if k == 0:
            got_stats[n] = flat
        else:
            share_stats[n] = flat
            for c in share_copy(head, k):
                c.start()

    def combine(head):
        base = head * X_RING
        for k in range(1, X_RING):
            for c in share_copy(head, k):
                c.wait_recv()
        lse = [got_stats[base + k] for k in range(X_RING)]
        peak = functools.reduce(jnp.maximum, lse)
        weight = [jnp.exp2(v - peak) for v in lse]
        row = lax.broadcasted_iota(jnp.int32, peak.shape, 0)
        factor = jnp.where(row == 1, -(subtract_wide if head else subtract_narrow)[0], 1.0) / functools.reduce(jnp.add, weight)
        wide = jnp.concatenate(
            [w * factor for w in weight]
            + [jnp.zeros((128 - 8 * X_RING, peak.shape[1]), jnp.float32)],
            0,
        )
        turned = jnp.transpose(wide)[0:tok]
        diff = jnp.zeros((tok, 128), jnp.float32)
        for k in range(X_RING):
            o = got[base + k].astype(jnp.float32)
            for m in range(2):
                diff = diff + turned[:, 8 * k + m : 8 * k + m + 1] * o[:, 128 * m : 128 * m + 128]
        spread = jnp.mean(diff * diff, -1, keepdims=True)
        normed = diff * lax.rsqrt(spread + 1e-06) * head_gain[...]
        attended[head] = normed.reshape(heads, tok // heads, 128).astype(jnp.bfloat16)

    pass_on_keys(1, 0)
    start_step(1, 2)
    query_copies[3].wait_recv()
    query_copies[1].wait_recv()
    absorb(0, 1, 0, 768)
    pass_on_keys(2, 0)
    pass_on_keys(1, 1)
    query_copies[2].wait_recv()
    absorb(0, 0, 0, 768)
    arrived(1, 2)
    absorb_both(1, 0, 768)
    pass_on_keys(3, 0)
    start_step(2, 2)
    absorb(0, 0, 768, 768)
    pass_on_keys(2, 1)
    absorb(0, 1, 768, 768)
    absorb_both(0, 1536, 512)
    arrived(4, 0)
    absorb(0, 0, 2048, 512)
    arrived(2, 2)
    start_step(3, 2)
    finish(0, 2)
    finish(0, 1)
    absorb(0, 1, 2048, 512)
    finish(0, 3)
    pass_on_keys(3, 1)
    finish(0, 0)
    absorb_both(1, 768, 768)
    arrived(3, 2)
    absorb_both(1, 1536, 512)
    arrived(4, 1)
    absorb(1, 0, 2048, 512)
    finish(1, 2)
    finish(1, 1)
    absorb(1, 1, 2048, 512)
    finish(1, 3)
    finish(1, 0)

    def head_copy(head, k):
        return remote(
            attended.at[head, lax.rem(tp + k, heads)], gathered_heads.at[head, tp],
            a_send.at[head, k], a_recv.at[head, k], along_tp(k),
        )

    def send_heads(head):
        combine(head)
        for k in range(1, heads):
            head_copy(head, k).start()
        gathered_heads[head, pl.ds(tp, 1)] = attended[head, pl.ds(tp, 1)]

    def project(head, weight):
        for k in range(1, heads):
            head_copy(head, k).wait_recv()
        all_heads = jnp.concatenate([gathered_heads[head, t] for t in range(heads)], 1)
        return jnp.dot(all_heads, weight[...], preferred_element_type=jnp.float32)

    send_heads(0)
    weights[0].wait()
    weights[1].wait()
    mix = project(0, mix_narrow)
    send_heads(1)
    mix = mix + project(1, mix_wide)
    hidden[...] = layer_norm(
        residual_scale * residual[...].astype(jnp.float32) + mix, norm1_gain[...]
    ).astype(jnp.bfloat16)

    y, core = tp // 2, tp % 2
    width = hidden.shape[1]
    half = width // 2
    f32, bf16 = jnp.float32, jnp.bfloat16

    def along_y(k):
        return (sp, lax.rem(y + k, Y_RING) * 2 + core)

    sibling = (sp, y * 2 + 1 - core)
    table = functools.reduce(jnp.add, [picks[c] for c in range(top_count)])
    rows = jnp.dot(table, hidden[...], preferred_element_type=f32)
    to_tiles(rows, words, outgoing, 0)

    def place(dz, dx):
        return dz % Z_RING * X_RING + dx % X_RING

    def dispatch_copy(g, dz, dx):
        e = expert_at(dz, dx)
        p = place(-dz, -dx)
        return remote(
            outgoing.at[g * experts + e], received.at[g * experts + p],
            d_send.at[g, p], d_recv.at[g, p], (e, tp),
        )

    def return_copy(g, dz, dx):
        p = place(dz, dx)
        return remote(
            results.at[g * experts + p], returned.at[g * experts + sp],
            r_send.at[g, p], r_recv.at[g, p], (expert_at(dz, dx), tp),
        )

    block = experts
    low, high = pl.ds(0, half), pl.ds(half, half)

    for g in range(capacity):
        for dz, dx in others:
            dispatch_copy(g, dz, dx).start()

    def gather_copies(g):
        at = lambda s, c=None: gathered.at[g, s] if c is None else gathered.at[g, s, :, c]
        right, left = along_y(1), along_y(Y_RING - 1)
        plan = {
            "core0": (at(0), at(1), sibling),
            "right": (at(0), at(6), right),
            "left": (at(0), at(2), left),
            "right2": (at(6, low), at(4, low), right),
            "left2": (at(2, high), at(4, high), left),
            "core1": (at(2), at(3), sibling),
            "core3": (at(6), at(7), sibling),
            "core2": (at(4), at(5), sibling),
        }
        return {
            name: remote(src, dst, g_send.at[g, i], g_recv.at[g, i], peer)
            for i, (name, (src, dst, peer)) in enumerate(plan.items())
        }

    gathers = [gather_copies(g) for g in range(capacity)]

    def core_copy(g, k):
        return remote(
            partial.at[g, 2 * k + 1], from_core.at[g, k], c_send.at[g, k], c_recv.at[g, k], sibling
        )

    def half_copy(g, way):
        return remote(
            half_sum.at[g, way], from_half.at[g, way], h_send.at[g, way], h_recv.at[g, way],
            along_y(Y_RING - 1 if way else 1),
        )

    def side_copy(g, way, part):
        cols = high if part else low
        return remote(
            whole_sum.at[g, way, :, cols], from_side.at[g, way, :, cols],
            f_send.at[g, way, part], f_recv.at[g, way, part], along_y(Y_RING - 1 if way else 1),
        )

    def open_group(g):
        received[g * experts] = outgoing[g * experts + sp]
        for dz, dx in others:
            dispatch_copy(g, -dz % Z_RING, -dx % X_RING).wait_recv()
        from_tiles(received, g * block, block, words, gathered.at[g, 0])
        for name in ("right", "left", "core0"):
            gathers[g][name].start()

    def pass_on(g):
        gathers[g]["right"].wait_recv()
        gathers[g]["right2"].start()
        gathers[g]["left"].wait_recv()
        gathers[g]["left2"].start()
        gathers[g]["core3"].start()
        gathers[g]["core1"].start()

    def close_gather(g):
        gathers[g]["right2"].wait_recv()
        gathers[g]["left2"].wait_recv()
        gathers[g]["core2"].start()
        for name in ("core0", "core1", "core3", "core2"):
            gathers[g][name].wait_recv()

    def multiply(g):
        flat = gathered[g].reshape(-1, width)
        gate_part = jnp.dot(flat, gate[...], preferred_element_type=f32)
        up_part = jnp.dot(flat, up[...], preferred_element_type=f32)
        inner = (gate_part * jax.nn.sigmoid(gate_part) * up_part).astype(bf16)
        share = jnp.dot(inner, down[...], preferred_element_type=f32).astype(bf16)
        partial[g] = share.reshape(2 * Y_RING, block, width)
        for k in (2, 1, 3, 0):
            core_copy(g, k).start()

    def both_cores(g, k, cols):
        return partial[g, 2 * k, :, cols].astype(f32) + from_core[g, k, :, cols].astype(f32)

    def send_halves(g):
        core_copy(g, 2).wait_recv()
        half_sum[g, 0] = both_cores(g, 2, low).astype(bf16)
        half_sum[g, 1] = both_cores(g, 2, high).astype(bf16)
        half_copy(g, 0).start()
        half_copy(g, 1).start()
        core_copy(g, 1).wait_recv()
        whole_sum[g, 0, :, high] = both_cores(g, 1, high).astype(bf16)
        side_copy(g, 0, 1).start()
        core_copy(g, 3).wait_recv()
        whole_sum[g, 1, :, low] = both_cores(g, 3, low).astype(bf16)
        side_copy(g, 1, 0).start()

    def send_sides(g):
        half_copy(g, 0).wait_recv()
        whole_sum[g, 0, :, low] = (both_cores(g, 1, low) + from_half[g, 0].astype(f32)).astype(bf16)
        side_copy(g, 0, 0).start()
        half_copy(g, 1).wait_recv()
        whole_sum[g, 1, :, high] = (both_cores(g, 3, high) + from_half[g, 1].astype(f32)).astype(
            bf16
        )
        side_copy(g, 1, 1).start()

    def give_back(g):
        core_copy(g, 0).wait_recv()
        for way in range(2):
            for part in range(2):
                side_copy(g, way, part).wait_recv()
        total = (
            both_cores(g, 0, slice(None))
            + from_side[g, 0].astype(f32)
            + from_side[g, 1].astype(f32)
        )
        to_tiles(total, words, results, g * block)
        for dz, dx in others:
            return_copy(g, dz, dx).start()
        returned[g * experts + sp] = results[g * experts]

    open_group(0)
    open_group(1)
    pass_on(0)
    open_group(2)
    pass_on(1)
    for c in weights[2:]:
        c.wait()
    close_gather(0)
    multiply(0)
    pass_on(2)
    send_halves(0)
    close_gather(1)
    multiply(1)
    send_sides(0)
    send_halves(1)
    close_gather(2)
    multiply(2)
    give_back(0)
    send_sides(1)
    send_halves(2)
    give_back(1)
    send_sides(2)
    give_back(2)
    for g in range(capacity):
        for dz, dx in others:
            return_copy(g, -dz % Z_RING, -dx % X_RING).wait_recv()
    from_tiles(returned, 0, experts * capacity, words, returned_rows)
    routed = jnp.zeros((local_rows, width), f32)
    for c in range(top_count):
        picked = lax.dot_general(
            picks[c], returned_rows[...], (((0,), (0,)), ((), ())), preferred_element_type=f32
        )
        routed = routed + scales[c, :, 0:1] * picked
    out[...] = layer_norm(
        residual_scale * hidden[...].astype(f32) + routed, norm2_gain[...]
    ).astype(bf16)
    for g in range(capacity):
        for dz, dx in others:
            dispatch_copy(g, dz, dx).wait_send()
            return_copy(g, dz, dx).wait_send()
        for c in gathers[g].values():
            c.wait_send()
        for k in range(Y_RING):
            core_copy(g, k).wait_send()
        for way in range(2):
            half_copy(g, way).wait_send()
            for part in range(2):
                side_copy(g, way, part).wait_send()
    for c in ring.values():
        c.wait_send()
    for c in query_copies.values():
        c.wait_send()
    for head in range(2):
        for k in range(1, X_RING):
            for c in share_copy(head, k):
                c.wait_send()
    for head in range(2):
        for k in range(1, heads):
            head_copy(head, k).wait_send()


def on_device(
    residual,
    query_narrow,
    key_narrow,
    value_narrow,
    query_wide,
    key_wide,
    value_wide,
    subtract_narrow,
    subtract_wide,
    head_gain,
    out_narrow,
    out_wide,
    norm1_gain,
    norm2_gain,
    expert_ids,
    expert_weight,
    gate_proj,
    up_proj,
    down_proj,
):
    tok = query_narrow.shape[0]
    heads = lax.axis_size("tp")
    lanes = (tok + 127) // 128 * 128
    local_rows, width = residual.shape
    experts = Z_RING * X_RING
    capacity = max(2, 3 * local_rows * expert_ids.shape[1] // (2 * experts))
    inner = gate_proj.shape[2]
    count = experts * capacity
    block = experts
    tall = width // LANES
    vmem = pl.BlockSpec(memory_space=pltpu.VMEM)
    smem = pl.BlockSpec(memory_space=pltpu.SMEM)
    hbm = pl.BlockSpec(memory_space=pl.ANY)
    dma = pltpu.SemaphoreType.DMA
    bf16, f32 = jnp.bfloat16, jnp.float32
    return pl.pallas_call(
        functools.partial(layer_kernel, tok, capacity),
        out_shape=jax.ShapeDtypeStruct((local_rows, width), bf16),
        in_specs=[vmem] + [hbm] * 6 + [smem] * 2 + [vmem] + [hbm] * 2 + [vmem] * 4 + [hbm] * 3,
        out_specs=vmem,
        scratch_shapes=[
            pltpu.VMEM((X_RING * tok, 384), bf16),
            pltpu.VMEM((Z_RING * tok, ROW), bf16),
            pltpu.VMEM((4, X_RING * tok, 128), f32),
            pltpu.VMEM((4, X_RING * tok, 256), f32),
            pltpu.VMEM((lanes, 128), f32),
            pltpu.VMEM((2 * X_RING, tok, 256), bf16),
            pltpu.VMEM((2 * X_RING, 8, lanes), f32),
            pltpu.VMEM((2 * X_RING, tok, 256), bf16),
            pltpu.VMEM((2 * X_RING, 8, lanes), f32),
            pltpu.VMEM((2, heads, tok // heads, 128), bf16),
            pltpu.VMEM((2, heads, tok // heads, 128), bf16),
            pltpu.VMEM(out_narrow.shape, bf16),
            pltpu.VMEM(out_wide.shape, bf16),
            pltpu.VMEM(residual.shape, bf16),
            pltpu.VMEM((expert_ids.shape[1], count, local_rows), bf16),
            pltpu.VMEM((expert_ids.shape[1], local_rows, LANES), f32),
            pltpu.VMEM((width, inner), bf16),
            pltpu.VMEM((width, inner), bf16),
            pltpu.VMEM((inner, width), bf16),
            pltpu.VMEM((count * tall, LANES), f32),
            pltpu.VMEM((count, tall, LANES), bf16),
            pltpu.VMEM((count, tall, LANES), bf16),
            pltpu.VMEM((capacity, 2 * Y_RING, block, width), bf16),
            pltpu.VMEM((capacity, 2 * Y_RING, block, width), bf16),
            pltpu.VMEM((capacity, Y_RING, block, width), bf16),
            pltpu.VMEM((capacity, 2, block, width // 2), bf16),
            pltpu.VMEM((capacity, 2, block, width // 2), bf16),
            pltpu.VMEM((capacity, 2, block, width), bf16),
            pltpu.VMEM((capacity, 2, block, width), bf16),
            pltpu.VMEM((count, tall, LANES), bf16),
            pltpu.VMEM((count, tall, LANES), bf16),
            pltpu.VMEM((count, width), bf16),
            dma((6,)),
            dma((X_RING,)),
            dma((X_RING,)),
            dma((3 * Z_RING,)),
            dma((3 * Z_RING,)),
            dma((2 * X_RING,)),
            dma((2 * X_RING,)),
            dma((2 * X_RING,)),
            dma((2 * X_RING,)),
            dma((2, heads)),
            dma((2, heads)),
            dma((5,)),
            dma((capacity, experts)),
            dma((capacity, experts)),
            dma((capacity, 8)),
            dma((capacity, 8)),
            dma((capacity, Y_RING)),
            dma((capacity, Y_RING)),
            dma((capacity, 2)),
            dma((capacity, 2)),
            dma((capacity, 2, 2)),
            dma((capacity, 2, 2)),
            dma((capacity, experts)),
            dma((capacity, experts)),
        ],
        compiler_params=pltpu.CompilerParams(
            collective_id=0, has_side_effects=True, vmem_limit_bytes=66 * 1000 * 1000
        ),
        name="layer",
    )(
        residual, query_narrow, key_narrow, value_narrow, query_wide, key_wide, value_wide,
        subtract_narrow, subtract_wide, head_gain.reshape(1, -1), out_narrow, out_wide,
        norm1_gain.reshape(1, -1), norm2_gain.reshape(1, -1), jnp.transpose(expert_ids),
        jnp.transpose(expert_weight), gate_proj, up_proj, down_proj,
    )


def solution(mesh):
    placed = (
        P(("sp", "tp"), None),
        P("sp", "tp"),
        P("sp", "tp"),
        P("sp", "tp"),
        P("sp", "tp"),
        P("sp", "tp"),
        P("sp", "tp"),
        P("tp"),
        P("tp"),
        P(),
        P(),
        P(),
        P(),
        P(),
        P(("sp", "tp"), None),
        P(("sp", "tp"), None),
        P("sp", None, "tp"),
        P("sp", None, "tp"),
        P("sp", "tp", None),
    )
    return jax.shard_map(
        on_device, mesh=mesh, in_specs=placed, out_specs=P(("sp", "tp"), None), check_vma=False
    )
```

```python
import functools

import jax
import jax.numpy as jnp
from jax import lax
from jax.experimental import pallas as pl
from jax.experimental.pallas import tpu as pltpu
from jax.sharding import PartitionSpec as P

residual_scale = 2.0**0.5
MESH = pl.DeviceIdType.MESH


def layer_norm(values, gain):
    center = jnp.mean(values, -1, keepdims=True)
    spread = jnp.mean(jnp.square(values - center), -1, keepdims=True)
    return (values - center) * lax.rsqrt(spread + 1e-05) * gain


LOG2E = 1.4426950408889634
Z_RING = 8
X_RING = 4
NARROW = (128, 384)
WIDE = (384, 768)
ROW = 896
PLACE = (0, 1, 3, 5, 7, 6, 4, 2)
QPLACE = (3, 1, 0, 2)


Y_RING = 4
LANES = 128


def to_tiles(values, words, target, first):
    rows, width = values.shape
    tall = width // LANES
    for j in range(tall):
        words[pl.ds(j, rows, stride=tall), :] = values[:, LANES * j : LANES * (j + 1)]
    flat = words[0 : rows * tall, :]
    target[first : first + rows] = flat.reshape(rows, tall, LANES).astype(jnp.bfloat16)


def from_tiles(source, first, rows, words, target):
    tall = source.shape[1]
    flat = source[first : first + rows].astype(jnp.float32)
    words[0 : rows * tall, :] = flat.reshape(rows * tall, LANES)
    for j in range(tall):
        target[:, LANES * j : LANES * (j + 1)] = words[pl.ds(j, rows, stride=tall), :].astype(
            jnp.bfloat16
        )


def layer_kernel(
    tok,
    capacity,
    residual,
    query_narrow,
    key_narrow,
    value_narrow,
    query_wide,
    key_wide,
    value_wide,
    subtract_narrow,
    subtract_wide,
    head_gain,
    out_narrow,
    out_wide,
    norm1_gain,
    norm2_gain,
    expert_ids,
    expert_weight,
    gate_proj,
    up_proj,
    down_proj,
    out,
    queries,
    keys,
    top,
    acc,
    stats,
    share,
    share_stats,
    got,
    got_stats,
    attended,
    gathered_heads,
    mix_narrow,
    mix_wide,
    hidden,
    picks,
    scales,
    gate,
    up,
    down,
    words,
    outgoing,
    received,
    gathered,
    partial,
    from_core,
    half_sum,
    from_half,
    whole_sum,
    from_side,
    results,
    returned,
    returned_rows,
    local_sem,
    q_send,
    q_recv,
    kv_send,
    kv_recv,
    o_send,
    o_recv,
    s_send,
    s_recv,
    a_send,
    a_recv,
    w_sem,
    d_send,
    d_recv,
    g_send,
    g_recv,
    c_send,
    c_recv,
    h_send,
    h_recv,
    f_send,
    f_recv,
    r_send,
    r_recv,
):
    sp = lax.axis_index("sp")
    tp = lax.axis_index("tp")
    heads = lax.axis_size("tp")
    z, x = sp // X_RING, sp % X_RING

    def along_z(k):
        return (lax.rem(z + k, Z_RING) * X_RING + x, tp)

    def along_x(k):
        return (z * X_RING + lax.rem(x + k, X_RING), tp)

    def along_tp(k):
        return (sp, lax.rem(tp + k, heads))

    def expert_at(dz, dx):
        return lax.rem(z + dz, Z_RING) * X_RING + lax.rem(x + dx, X_RING)

    own_q = QPLACE[0] * tok
    loads = [
        pltpu.make_async_copy(src, dst, local_sem.at[i])
        for i, (src, dst) in enumerate(
            (
                (query_narrow, queries.at[pl.ds(own_q, tok), pl.ds(0, 128)]),
                (query_wide, queries.at[pl.ds(own_q, tok), pl.ds(128, 256)]),
                (value_narrow, keys.at[pl.ds(0, tok), pl.ds(128, 128)]),
                (key_narrow, keys.at[pl.ds(0, tok), pl.ds(256, 128)]),
                (key_wide, keys.at[pl.ds(0, tok), pl.ds(384, 256)]),
                (value_wide, keys.at[pl.ds(0, tok), pl.ds(640, 128)]),
            )
        )
    ]
    for c in loads:
        c.start()

    weights = [
        pltpu.make_async_copy(src, dst, w_sem.at[i])
        for i, (src, dst) in enumerate(
            (
                (out_narrow, mix_narrow),
                (out_wide, mix_wide),
                (gate_proj.at[0], gate),
                (up_proj.at[0], up),
                (down_proj.at[0], down),
            )
        )
    ]
    others = [(dz, dx) for dz in (4, 3, 5, 2, 6, 1, 7, 0) for dx in range(X_RING) if dz or dx]
    barrier = pltpu.get_barrier_semaphore()
    peers = [along_z(1), along_z(Z_RING - 1)] + [along_x(k) for k in range(1, X_RING)]
    peers = peers + [along_tp(k) for k in range(1, heads)]
    for peer in peers:
        pl.semaphore_signal(barrier, inc=1, device_id=peer, device_id_type=MESH)
    keys[:, 0:128] = jnp.ones((keys.shape[0], 128), jnp.bfloat16)
    keys[:, 768:896] = jnp.ones((keys.shape[0], 128), jnp.bfloat16)
    top[...] = jnp.full(top.shape, -1e30, jnp.float32)
    acc[...] = jnp.zeros(acc.shape, jnp.float32)
    stats[...] = jnp.zeros(stats.shape, jnp.float32)
    for c in loads:
        c.wait()
    pl.semaphore_wait(barrier, len(peers))

    def remote(src, dst, send, recv, peer):
        return pltpu.make_async_remote_copy(
            src_ref=src, dst_ref=dst, send_sem=send, recv_sem=recv, device_id=peer,
            device_id_type=MESH,
        )

    top_count, local_rows = expert_ids.shape
    experts = Z_RING * X_RING

    def choose():
        lane = lax.broadcasted_iota(jnp.int32, (experts, local_rows), 0)
        named = [(expert_ids[c : c + 1, :] == lane).astype(jnp.float32) for c in range(top_count)]
        i = lax.broadcasted_iota(jnp.int32, (local_rows, local_rows), 0)
        j = lax.broadcasted_iota(jnp.int32, (local_rows, local_rows), 1)
        earlier = (i < j).astype(jnp.float32).astype(jnp.bfloat16)
        before = jnp.dot(
            functools.reduce(jnp.add, named).astype(jnp.bfloat16), earlier,
            preferred_element_type=jnp.float32,
        )
        row = lax.broadcasted_iota(jnp.int32, (experts * capacity, local_rows), 0)
        for c in range(top_count):
            position = jnp.sum(before * named[c], 0, keepdims=True)
            slot = position * experts + expert_ids[c : c + 1, :].astype(jnp.float32)
            picks[c] = (slot == row.astype(jnp.float32)).astype(jnp.float32).astype(jnp.bfloat16)
            before = before + named[c]
            own = jnp.where(i == j, expert_weight[c : c + 1, :], 0.0)
            scales[c] = jnp.broadcast_to(jnp.sum(own, 1, keepdims=True), scales.shape[1:])

    def ring_copy(way, step, piece):
        cols = WIDE if piece else NARROW
        forward = way == 0
        source = (Z_RING - step + 1) % Z_RING if forward else step - 1
        target = (Z_RING - step) % Z_RING if forward else step
        r0, rows = 0, tok
        if piece or 2 * step == Z_RING:
            rows = tok // 2
            r0 = 0 if forward == (piece < 2) else rows
        at = lambda k: keys.at[
            pl.ds(PLACE[k] * tok + r0, rows), pl.ds(cols[0], cols[1] - cols[0])
        ]
        n = (way * (Z_RING // 2) + step - 1) * 3 + piece
        return remote(
            at(source), at(target), kv_send.at[n], kv_recv.at[n],
            along_z(1 if forward else Z_RING - 1),
        )

    def query_copy(k):
        return remote(
            queries.at[pl.ds(own_q, tok), :],
            queries.at[pl.ds(QPLACE[(X_RING - k) % X_RING] * tok, tok), :],
            q_send.at[k], q_recv.at[k], along_x(k),
        )

    ring = {
        (w, s, p): ring_copy(w, s, p)
        for w in range(2)
        for s in range(1, Z_RING // 2 + 1)
        for p in range(3 if 2 * s < Z_RING else 2)
    }
    query_copies = {k: query_copy(k) for k in range(1, X_RING)}

    def start_step(step, piece):
        for w in range(2):
            ring[w, step, piece].start()

    def arrived(step, piece):
        for w in range(2):
            ring[w, step, piece].wait_recv()

    def pass_on_keys(step, piece):
        for w in range(2):
            ring[w, step, piece].wait_recv()
            ring[w, step + 1, piece].start()

    start_step(1, 0)
    for k in (1, 3, 2):
        query_copies[k].start()
    start_step(1, 1)
    for c in weights:
        c.start()
    choose()

    pair = 2 * tok

    def absorb(head, group, k0, span):
        rows = pl.ds(k0, span)
        qrows = pl.ds(group * pair, pair)
        size = 128 if head else 64
        scale = size**-0.5 * LOG2E
        scores = []
        for m in range(2):
            if head:
                q = queries[qrows, 128 + 128 * m : 256 + 128 * m]
                k = keys[rows, 384 + 128 * m : 512 + 128 * m]
            else:
                q = queries[qrows, 0:128]
                lane = lax.broadcasted_iota(jnp.int32, q.shape, 1)
                q = jnp.where((lane < 64) if m == 0 else (lane >= 64), q, jnp.zeros_like(q))
                k = keys[rows, 256:384]
            scores.append(
                lax.dot_general(
                    q, k, (((1,), (1,)), ((), ())), preferred_element_type=jnp.float32
                )
            )
        v = keys[rows, 640:896] if head else keys[rows, 0:256]
        for m in range(2):
            s = scores[m]
            before = top[2 * head + m, qrows, :]
            now = jnp.maximum(before, jnp.max(s, -1, keepdims=True) * scale)
            expo = jnp.exp2(s * scale - now[:, :1])
            shrink = jnp.exp2(before - now)
            add = jnp.dot(expo.astype(jnp.bfloat16), v, preferred_element_type=jnp.float32)
            a = acc[2 * head + m, qrows, :]
            acc[2 * head + m, qrows, :] = (
                jnp.concatenate([a[:, :128] * shrink, a[:, 128:] * shrink], 1) + add
            )
            top[2 * head + m, qrows, :] = now

    def absorb_both(head, k0, span):
        def one(g, carry):
            absorb(head, g, k0, span)
            return carry

        lax.fori_loop(0, 2, one, 0)

    def share_copy(head, k):
        to = (X_RING - k) % X_RING
        n = head * X_RING + k
        return (
            remote(share.at[n], got.at[head * X_RING + to], o_send.at[n], o_recv.at[n], along_x(k)),
            remote(
                share_stats.at[n], got_stats.at[head * X_RING + to], s_send.at[n], s_recv.at[n],
                along_x(k),
            ),
        )

    def finish(head, k):
        n = head * X_RING + k
        qrows = pl.ds(QPLACE[k] * tok, tok)
        lane = lax.broadcasted_iota(jnp.int32, (tok, 128), 1)
        column = jnp.zeros((tok, 128), jnp.float32)
        parts = []
        for m in range(2):
            a = acc[2 * head + m, qrows, :]
            value, total = (a[:, :128], a[:, 128:]) if head else (a[:, 128:], a[:, :128])
            parts.append(value / total)
            column = jnp.where(lane == m, top[2 * head + m, qrows, :] + jnp.log2(total), column)
        both = jnp.concatenate(parts, 1)
        if k == 0:
            got[n] = both.astype(jnp.bfloat16)
        else:
            share[n] = both.astype(jnp.bfloat16)
        stats[0:tok, :] = column
        flat = jnp.transpose(stats[...])[0:8]
        if k == 0:
            got_stats[n] = flat
        else:
            share_stats[n] = flat
            for c in share_copy(head, k):
                c.start()

    def combine(head):
        base = head * X_RING
        for k in range(1, X_RING):
            for c in share_copy(head, k):
                c.wait_recv()
        lse = [got_stats[base + k] for k in range(X_RING)]
        peak = functools.reduce(jnp.maximum, lse)
        weight = [jnp.exp2(v - peak) for v in lse]
        row = lax.broadcasted_iota(jnp.int32, peak.shape, 0)
        factor = jnp.where(row == 1, -(subtract_wide if head else subtract_narrow)[0], 1.0) / functools.reduce(jnp.add, weight)
        wide = jnp.concatenate(
            [w * factor for w in weight]
            + [jnp.zeros((128 - 8 * X_RING, peak.shape[1]), jnp.float32)],
            0,
        )
        turned = jnp.transpose(wide)[0:tok]
        diff = jnp.zeros((tok, 128), jnp.float32)
        for k in range(X_RING):
            o = got[base + k].astype(jnp.float32)
            for m in range(2):
                diff = diff + turned[:, 8 * k + m : 8 * k + m + 1] * o[:, 128 * m : 128 * m + 128]
        spread = jnp.mean(diff * diff, -1, keepdims=True)
        normed = diff * lax.rsqrt(spread + 1e-06) * head_gain[...]
        attended[head] = normed.reshape(heads, tok // heads, 128).astype(jnp.bfloat16)

    pass_on_keys(1, 0)
    start_step(1, 2)
    query_copies[3].wait_recv()
    query_copies[1].wait_recv()
    absorb(0, 1, 0, 768)
    pass_on_keys(2, 0)
    pass_on_keys(1, 1)
    query_copies[2].wait_recv()
    absorb(0, 0, 0, 768)
    arrived(1, 2)
    absorb_both(1, 0, 768)
    pass_on_keys(3, 0)
    start_step(2, 2)
    absorb(0, 0, 768, 768)
    pass_on_keys(2, 1)
    absorb(0, 1, 768, 768)
    absorb_both(0, 1536, 512)
    arrived(4, 0)
    absorb(0, 0, 2048, 512)
    arrived(2, 2)
    start_step(3, 2)
    finish(0, 2)
    finish(0, 1)
    absorb(0, 1, 2048, 512)
    finish(0, 3)
    pass_on_keys(3, 1)
    finish(0, 0)
    absorb_both(1, 768, 768)
    arrived(3, 2)
    absorb_both(1, 1536, 512)
    arrived(4, 1)
    absorb(1, 0, 2048, 512)
    finish(1, 2)
    finish(1, 1)
    absorb(1, 1, 2048, 512)
    finish(1, 3)
    finish(1, 0)

    def head_copy(head, k):
        return remote(
            attended.at[head, lax.rem(tp + k, heads)], gathered_heads.at[head, tp],
            a_send.at[head, k], a_recv.at[head, k], along_tp(k),
        )

    def send_heads(head):
        combine(head)
        for k in sorted(range(1, heads), key=lambda k: abs(k - heads // 2)):
            head_copy(head, k).start()
        gathered_heads[head, pl.ds(tp, 1)] = attended[head, pl.ds(tp, 1)]

    def project(head, weight):
        for k in range(1, heads):
            head_copy(head, k).wait_recv()
        all_heads = jnp.concatenate([gathered_heads[head, t] for t in range(heads)], 1)
        return jnp.dot(all_heads, weight[...], preferred_element_type=jnp.float32)

    send_heads(0)
    weights[0].wait()
    weights[1].wait()
    mix = project(0, mix_narrow)
    send_heads(1)
    mix = mix + project(1, mix_wide)
    hidden[...] = layer_norm(
        residual_scale * residual[...].astype(jnp.float32) + mix, norm1_gain[...]
    ).astype(jnp.bfloat16)

    y, core = tp // 2, tp % 2
    width = hidden.shape[1]
    half = width // 2
    f32, bf16 = jnp.float32, jnp.bfloat16

    def along_y(k):
        return (sp, lax.rem(y + k, Y_RING) * 2 + core)

    sibling = (sp, y * 2 + 1 - core)
    def place(dz, dx):
        return dz % Z_RING * X_RING + dx % X_RING

    def dispatch_copy(g, dz, dx):
        e = expert_at(dz, dx)
        p = place(-dz, -dx)
        return remote(
            outgoing.at[g * experts + e], received.at[g * experts + p],
            d_send.at[g, p], d_recv.at[g, p], (e, tp),
        )

    def return_copy(g, dz, dx):
        p = place(dz, dx)
        return remote(
            results.at[g * experts + p], returned.at[g * experts + sp],
            r_send.at[g, p], r_recv.at[g, p], (expert_at(dz, dx), tp),
        )

    block = experts
    low, high = pl.ds(0, half), pl.ds(half, half)

    for g in range(capacity):
        part = pl.ds(g * experts, experts)
        table = functools.reduce(jnp.add, [picks[c, part] for c in range(top_count)])
        rows = jnp.dot(table, hidden[...], preferred_element_type=f32)
        to_tiles(rows, words, outgoing, g * experts)
        for dz, dx in others:
            dispatch_copy(g, dz, dx).start()

    def gather_copies(g):
        at = lambda s, c=None: gathered.at[g, s] if c is None else gathered.at[g, s, :, c]
        right, left = along_y(1), along_y(Y_RING - 1)
        plan = {
            "core0": (at(0), at(1), sibling),
            "right": (at(0), at(6), right),
            "left": (at(0), at(2), left),
            "right2": (at(6, low), at(4, low), right),
            "left2": (at(2, high), at(4, high), left),
            "core1": (at(2), at(3), sibling),
            "core3": (at(6), at(7), sibling),
            "core2": (at(4), at(5), sibling),
        }
        return {
            name: remote(src, dst, g_send.at[g, i], g_recv.at[g, i], peer)
            for i, (name, (src, dst, peer)) in enumerate(plan.items())
        }

    gathers = [gather_copies(g) for g in range(capacity)]

    def core_copy(g, k):
        return remote(
            partial.at[g, 2 * k + 1], from_core.at[g, k], c_send.at[g, k], c_recv.at[g, k], sibling
        )

    def half_copy(g, way):
        return remote(
            half_sum.at[g, way], from_half.at[g, way], h_send.at[g, way], h_recv.at[g, way],
            along_y(Y_RING - 1 if way else 1),
        )

    def side_copy(g, way, part):
        cols = high if part else low
        return remote(
            whole_sum.at[g, way, :, cols], from_side.at[g, way, :, cols],
            f_send.at[g, way, part], f_recv.at[g, way, part], along_y(Y_RING - 1 if way else 1),
        )

    def open_group(g):
        received[g * experts] = outgoing[g * experts + sp]
        for dz, dx in others:
            dispatch_copy(g, -dz % Z_RING, -dx % X_RING).wait_recv()
        from_tiles(received, g * block, block, words, gathered.at[g, 0])
        for name in ("right", "left", "core0"):
            gathers[g][name].start()

    def pass_on(g):
        gathers[g]["right"].wait_recv()
        gathers[g]["right2"].start()
        gathers[g]["left"].wait_recv()
        gathers[g]["left2"].start()
        gathers[g]["core3"].start()
        gathers[g]["core1"].start()

    def close_gather(g):
        gathers[g]["right2"].wait_recv()
        gathers[g]["left2"].wait_recv()
        gathers[g]["core2"].start()
        multiply(g, (0, 2, 4, 6))
        for name in ("core0", "core1", "core3", "core2"):
            gathers[g][name].wait_recv()
        multiply(g, (5, 3, 7, 1))

    def multiply(g, slots):
        flat = jnp.concatenate([gathered[g, n] for n in slots], 0)
        gate_part = jnp.dot(flat, gate[...], preferred_element_type=f32)
        up_part = jnp.dot(flat, up[...], preferred_element_type=f32)
        inner = (gate_part * jax.nn.sigmoid(gate_part) * up_part).astype(bf16)
        share = jnp.dot(inner, down[...], preferred_element_type=f32).astype(bf16)
        for i, n in enumerate(slots):
            partial[g, n] = share[i * block : (i + 1) * block]
            if n % 2:
                core_copy(g, n // 2).start()

    def both_cores(g, k, cols):
        return partial[g, 2 * k, :, cols].astype(f32) + from_core[g, k, :, cols].astype(f32)

    def send_halves(g):
        core_copy(g, 2).wait_recv()
        half_sum[g, 0] = both_cores(g, 2, low).astype(bf16)
        half_sum[g, 1] = both_cores(g, 2, high).astype(bf16)
        half_copy(g, 0).start()
        half_copy(g, 1).start()
        core_copy(g, 1).wait_recv()
        whole_sum[g, 0, :, high] = both_cores(g, 1, high).astype(bf16)
        side_copy(g, 0, 1).start()
        core_copy(g, 3).wait_recv()
        whole_sum[g, 1, :, low] = both_cores(g, 3, low).astype(bf16)
        side_copy(g, 1, 0).start()

    def send_sides(g):
        half_copy(g, 0).wait_recv()
        whole_sum[g, 0, :, low] = (both_cores(g, 1, low) + from_half[g, 0].astype(f32)).astype(bf16)
        side_copy(g, 0, 0).start()
        half_copy(g, 1).wait_recv()
        whole_sum[g, 1, :, high] = (both_cores(g, 3, high) + from_half[g, 1].astype(f32)).astype(
            bf16
        )
        side_copy(g, 1, 1).start()

    def give_back(g):
        core_copy(g, 0).wait_recv()
        for way in range(2):
            for part in range(2):
                side_copy(g, way, part).wait_recv()
        total = (
            both_cores(g, 0, slice(None))
            + from_side[g, 0].astype(f32)
            + from_side[g, 1].astype(f32)
        )
        to_tiles(total, words, results, g * block)
        for dz, dx in others:
            return_copy(g, dz, dx).start()
        returned[g * experts + sp] = results[g * experts]

    open_group(0)
    open_group(1)
    pass_on(0)
    open_group(2)
    pass_on(1)
    for c in weights[2:]:
        c.wait()
    close_gather(0)
    pass_on(2)
    send_halves(0)
    close_gather(1)
    send_sides(0)
    send_halves(1)
    close_gather(2)
    give_back(0)
    send_sides(1)
    send_halves(2)
    give_back(1)
    send_sides(2)
    give_back(2)
    picked = [jnp.zeros((local_rows, width), f32) for c in range(top_count)]
    for g in range(capacity):
        for dz, dx in others:
            return_copy(g, -dz % Z_RING, -dx % X_RING).wait_recv()
        from_tiles(returned, g * experts, experts, words, returned_rows)
        for c in range(top_count):
            picked[c] = picked[c] + lax.dot_general(
                picks[c, pl.ds(g * experts, experts)], returned_rows[...],
                (((0,), (0,)), ((), ())), preferred_element_type=f32,
            )
    routed = jnp.zeros((local_rows, width), f32)
    for c in range(top_count):
        routed = routed + scales[c, :, 0:1] * picked[c]
    out[...] = layer_norm(
        residual_scale * hidden[...].astype(f32) + routed, norm2_gain[...]
    ).astype(bf16)
    for g in range(capacity):
        for dz, dx in others:
            dispatch_copy(g, dz, dx).wait_send()
            return_copy(g, dz, dx).wait_send()
        for c in gathers[g].values():
            c.wait_send()
        for k in range(Y_RING):
            core_copy(g, k).wait_send()
        for way in range(2):
            half_copy(g, way).wait_send()
            for part in range(2):
                side_copy(g, way, part).wait_send()
    for c in ring.values():
        c.wait_send()
    for c in query_copies.values():
        c.wait_send()
    for head in range(2):
        for k in range(1, X_RING):
            for c in share_copy(head, k):
                c.wait_send()
    for head in range(2):
        for k in range(1, heads):
            head_copy(head, k).wait_send()


def on_device(
    residual,
    query_narrow,
    key_narrow,
    value_narrow,
    query_wide,
    key_wide,
    value_wide,
    subtract_narrow,
    subtract_wide,
    head_gain,
    out_narrow,
    out_wide,
    norm1_gain,
    norm2_gain,
    expert_ids,
    expert_weight,
    gate_proj,
    up_proj,
    down_proj,
):
    tok = query_narrow.shape[0]
    heads = lax.axis_size("tp")
    lanes = (tok + 127) // 128 * 128
    local_rows, width = residual.shape
    experts = Z_RING * X_RING
    capacity = max(2, 3 * local_rows * expert_ids.shape[1] // (2 * experts))
    inner = gate_proj.shape[2]
    count = experts * capacity
    block = experts
    tall = width // LANES
    vmem = pl.BlockSpec(memory_space=pltpu.VMEM)
    smem = pl.BlockSpec(memory_space=pltpu.SMEM)
    hbm = pl.BlockSpec(memory_space=pl.ANY)
    dma = pltpu.SemaphoreType.DMA
    bf16, f32 = jnp.bfloat16, jnp.float32
    return pl.pallas_call(
        functools.partial(layer_kernel, tok, capacity),
        out_shape=jax.ShapeDtypeStruct((local_rows, width), bf16),
        in_specs=[vmem] + [hbm] * 6 + [smem] * 2 + [vmem] + [hbm] * 2 + [vmem] * 4 + [hbm] * 3,
        out_specs=vmem,
        scratch_shapes=[
            pltpu.VMEM((X_RING * tok, 384), bf16),
            pltpu.VMEM((Z_RING * tok, ROW), bf16),
            pltpu.VMEM((4, X_RING * tok, 128), f32),
            pltpu.VMEM((4, X_RING * tok, 256), f32),
            pltpu.VMEM((lanes, 128), f32),
            pltpu.VMEM((2 * X_RING, tok, 256), bf16),
            pltpu.VMEM((2 * X_RING, 8, lanes), f32),
            pltpu.VMEM((2 * X_RING, tok, 256), bf16),
            pltpu.VMEM((2 * X_RING, 8, lanes), f32),
            pltpu.VMEM((2, heads, tok // heads, 128), bf16),
            pltpu.VMEM((2, heads, tok // heads, 128), bf16),
            pltpu.VMEM(out_narrow.shape, bf16),
            pltpu.VMEM(out_wide.shape, bf16),
            pltpu.VMEM(residual.shape, bf16),
            pltpu.VMEM((expert_ids.shape[1], count, local_rows), bf16),
            pltpu.VMEM((expert_ids.shape[1], local_rows, LANES), f32),
            pltpu.VMEM((width, inner), bf16),
            pltpu.VMEM((width, inner), bf16),
            pltpu.VMEM((inner, width), bf16),
            pltpu.VMEM((count * tall, LANES), f32),
            pltpu.VMEM((count, tall, LANES), bf16),
            pltpu.VMEM((count, tall, LANES), bf16),
            pltpu.VMEM((capacity, 2 * Y_RING, block, width), bf16),
            pltpu.VMEM((capacity, 2 * Y_RING, block, width), bf16),
            pltpu.VMEM((capacity, Y_RING, block, width), bf16),
            pltpu.VMEM((capacity, 2, block, width // 2), bf16),
            pltpu.VMEM((capacity, 2, block, width // 2), bf16),
            pltpu.VMEM((capacity, 2, block, width), bf16),
            pltpu.VMEM((capacity, 2, block, width), bf16),
            pltpu.VMEM((count, tall, LANES), bf16),
            pltpu.VMEM((count, tall, LANES), bf16),
            pltpu.VMEM((experts, width), bf16),
            dma((6,)),
            dma((X_RING,)),
            dma((X_RING,)),
            dma((3 * Z_RING,)),
            dma((3 * Z_RING,)),
            dma((2 * X_RING,)),
            dma((2 * X_RING,)),
            dma((2 * X_RING,)),
            dma((2 * X_RING,)),
            dma((2, heads)),
            dma((2, heads)),
            dma((5,)),
            dma((capacity, experts)),
            dma((capacity, experts)),
            dma((capacity, 8)),
            dma((capacity, 8)),
            dma((capacity, Y_RING)),
            dma((capacity, Y_RING)),
            dma((capacity, 2)),
            dma((capacity, 2)),
            dma((capacity, 2, 2)),
            dma((capacity, 2, 2)),
            dma((capacity, experts)),
            dma((capacity, experts)),
        ],
        compiler_params=pltpu.CompilerParams(
            collective_id=0, has_side_effects=True, vmem_limit_bytes=66 * 1000 * 1000
        ),
        name="layer",
    )(
        residual, query_narrow, key_narrow, value_narrow, query_wide, key_wide, value_wide,
        subtract_narrow, subtract_wide, head_gain.reshape(1, -1), out_narrow, out_wide,
        norm1_gain.reshape(1, -1), norm2_gain.reshape(1, -1), jnp.transpose(expert_ids),
        jnp.transpose(expert_weight), gate_proj, up_proj, down_proj,
    )


def solution(mesh):
    placed = (
        P(("sp", "tp"), None),
        P("sp", "tp"),
        P("sp", "tp"),
        P("sp", "tp"),
        P("sp", "tp"),
        P("sp", "tp"),
        P("sp", "tp"),
        P("tp"),
        P("tp"),
        P(),
        P(),
        P(),
        P(),
        P(),
        P(("sp", "tp"), None),
        P(("sp", "tp"), None),
        P("sp", None, "tp"),
        P("sp", None, "tp"),
        P("sp", "tp", None),
    )
    return jax.shard_map(
        on_device, mesh=mesh, in_specs=placed, out_specs=P(("sp", "tp"), None), check_vma=False
    )
```
